256 devices in a mesh: sp: 32 (over z, x), tp: 8 (over y, core).
Axes of the slice: x: 4, y: 4, z: 8, core: 2. Of those that a mesh axis runs over, the one named last changes fastest.
Arguments:
- resid: bfloat16 [8192, 2048], P('sp'), may hold values from -6 to 6
- query_one: bfloat16 [8192, 1024], P('sp', 'tp'), may hold values from -400 to 400
- query_two: bfloat16 [8192, 1024], P('sp', 'tp'), may hold values from -400 to 400
- key_one: bfloat16 [8192, 1024], P('sp', 'tp'), may hold values from -8 to 8
- key_two: bfloat16 [8192, 1024], P('sp', 'tp'), may hold values from -8 to 8
- values: bfloat16 [8192, 2048], P('sp', 'tp'), may hold values from -6 to 6
- documents: int32 [8192], P('sp'), may hold values from 0 to 7, never falling along the last dimension, each value on 1 to 4352 neighbouring positions
- mix_lambda: float32 [16], P('tp'), may hold values from 0.3 to 0.8
- head_gain: float32 [128], replicated, may hold values from 0.1 to 1.9
- out_weight: bfloat16 [2048, 2048], P('tp'), may hold values from -0.125 to 0.125
- ffn_gain: float32 [2048], replicated, may hold values from 0.1 to 1.9
- routes: int32 [8192, 4], P('sp'), may hold values from 0 to 255, all different within a row; in each aligned block of 256 rows (0 to 255, 256 to 511, ...) at most 8 rows name the same one
- route_weight: float32 [8192, 4], P('sp'), may hold values from 0.2 to 0.9
- expert_gate: bfloat16 [256, 2048, 512], P(('sp', 'tp')), may hold values from -0.125 to 0.125
- expert_up: bfloat16 [256, 2048, 512], P(('sp', 'tp')), may hold values from -0.125 to 0.125
- expert_down: bfloat16 [256, 512, 2048], P(('sp', 'tp')), may hold values from -0.25 to 0.25
- shared_gate: bfloat16 [2048, 512], P(None, 'tp'), may hold values from -0.125 to 0.125
- shared_up: bfloat16 [2048, 512], P(None, 'tp'), may hold values from -0.125 to 0.125
- shared_down: bfloat16 [512, 2048], P('tp'), may hold values from -0.25 to 0.25
Outputs:
- layer_out: bfloat16 [8192, 2048], P(('sp', 'tp'))
The draws below stay inside these ranges and needn't reach their ends.
Inputs may be any that keep to these rules, and one draw needn't show every extreme that they name: `documents`: document numbers never fall along the positions; each document has 1 to 4352 positions and one has exactly 4352. `routes`: A row names 4 different experts. In each aligned block of 256 rows no expert is named by more than 8 rows, a bound that some block reaches.
All inputs are finite; a program needn't handle non-finite values.
Results may differ from the reference program's by a relative error of at most 0.018.
Values may be sent and summed in bfloat16 or wider, within the bound.
No kernel may reach another device: no remote copies, remote signals or barrier semaphores. Data moves between devices by JAX's collectives and lax.ppermute only.
A program may use at most 128 MiB of HBM per device.

```python
import math
from functools import partial
import jax
import jax.numpy as jnp
import numpy as np
from jax import lax

D = 2048
HEADS = 16
HEAD_DIM = 64
VAL_DIM = 128
EXP_FF = 512
SHARED_FF = 512
TOP = 4
TOK_DEV = 256
TOKENS = 8192
EXPERTS = 256
CAP = 8
DOC_COUNT = 8
DOC_MOST = 4352
N_SP = 32
N_TP = 8


def query_key_pair(key, which):
    base = jax.random.fold_in(key, 101 + which)
    key_query, key_keys = jax.random.split(base, 2)
    shape = (TOKENS, HEADS, HEAD_DIM)
    queries = jnp.clip(jax.random.normal(key_query, shape, jnp.float32) * 1.32, -8.0, 8.0)
    keyed = jnp.clip(jax.random.normal(key_keys, shape, jnp.float32) * 1.32, -8.0, 8.0)
    return (queries.reshape(TOKENS, HEADS * HEAD_DIM), keyed.reshape(TOKENS, HEADS * HEAD_DIM))


def draw_query_one(key, part):
    return query_key_pair(key, 1)[0].astype(jnp.bfloat16)


def draw_key_one(key, part):
    return query_key_pair(key, 1)[1].astype(jnp.bfloat16)


def draw_query_two(key, part):
    return query_key_pair(key, 2)[0].astype(jnp.bfloat16)


def draw_key_two(key, part):
    return query_key_pair(key, 2)[1].astype(jnp.bfloat16)


def steps_of(key, shape, shards, smallest, top_value):
    def one(position, parts):
        draws = jax.random.uniform(jax.random.fold_in(jax.random.fold_in(key, 6), position), (parts,), jnp.float32, smallest / len(shards), top_value / len(shards))
        return jnp.repeat(jnp.exp(draws), shape[position] // parts).reshape((-1,) + (1,) * (len(shape) - position - 1))

    level = one(*shards[0])
    for cut in shards[1:]:
        level = level * one(*cut)
    return level


def split_up(number_of, total, limit, lean):
    loads = [(1 << 20) // math.isqrt(rank ** lean) + 1 for rank in range(2, number_of + 1)]
    surplus, holding = total - limit - (number_of - 1), [1] * (number_of - 1)
    while surplus > 0:
        movable = [i for i in range(number_of - 1) if holding[i] < limit]
        whole, remaining = sum([loads[i] for i in movable]), surplus
        for i in movable:
            extra = min(limit - holding[i], max(1, remaining * loads[i] // whole), surplus)
            holding[i] = holding[i] + extra
            surplus = surplus - extra
    return np.array([limit] + holding)


def ragged(rng, amount, total, limit, skew):
    if amount == 2:
        one = jax.random.randint(rng, (), max(1, total - limit), min(limit, total - 1) + 1)
        return jnp.stack([one, total - one])
    sizes = jnp.asarray(split_up(amount, total, limit, skew), jnp.int32)
    twos = (amount - 1) // 2
    giver, taker = sizes[1:1 + 2 * twos:2], sizes[2:2 + 2 * twos:2]
    room = jnp.minimum(giver - 1, limit - taker)
    moved = jax.random.randint(jax.random.fold_in(rng, 1), (twos,), 0, 1 << 20) % (room + 1)
    sizes = sizes.at[1:1 + 2 * twos:2].set(giver - moved).at[2:2 + 2 * twos:2].set(taker + moved)
    return sizes[jax.random.permutation(jax.random.fold_in(rng, 2), amount)]


def deal_out(key, own, number, rows, count, top, most, lean):
    order = jax.random.permutation(key, count)
    packed, usual = load_shares(count, rows * top, most, lean, True), load_shares(count, rows * top, most, lean, False)
    places = jnp.arange(count)

    def named(tallies, offset_by):
        used = int((tallies > 0).sum())
        fixed = max(1, used // 4)
        shifted = fixed + (places - fixed + offset_by * (used - fixed)) % max(1, count - fixed)
        return jnp.zeros((count,), jnp.int32).at[order[jnp.where(places < fixed, places, shifted)]].set(jnp.asarray(tallies, jnp.int32))

    tallies = jnp.where(number % 4 == 0, named(packed, number // 4), named(usual, number - number // 4 - 1))
    mixed = jax.random.permutation(jax.random.fold_in(own, 3), count)
    giver, taker = mixed[0:count // 2 * 2:2], mixed[1:count // 2 * 2:2]
    slack = jnp.minimum(tallies[giver] - 1, most - tallies[taker]) // 2
    slack = jnp.where((giver == order[0]) | (taker == order[0]) | (tallies[taker] == 0), 0, jnp.maximum(slack, 0))
    shifted = jax.random.randint(jax.random.fold_in(own, 4), (count // 2,), 0, 1 << 20) % (slack + 1)
    tallies = tallies.at[giver].add(-shifted).at[taker].add(shifted)
    labels = jnp.searchsorted(jnp.cumsum(tallies), jnp.arange(rows * top), side="right").astype(jnp.int32)
    listing = labels.reshape(top, rows).T
    listing = listing[jax.random.permutation(jax.random.fold_in(own, 1), rows)]
    offset_by = jax.random.randint(jax.random.fold_in(own, 2), (rows, 1), 0, top)
    return jnp.take_along_axis(listing, (jnp.arange(top)[None, :] + offset_by) % top, axis=1)


def load_shares(amount, total, bound, lean, full):
    portions = [(1 << 20) // math.isqrt(rank ** lean) + 1 for rank in range(1, amount + 1)]
    largest = bound if full else min(bound, max(-(-total // amount), total * portions[0] // sum(portions)))
    least = 1 if total - largest >= amount - 1 else 0
    counts, spare = [largest] + [least] * (amount - 1), total - largest - least * (amount - 1)
    while spare > 0:
        free = [i for i in range(1, amount) if counts[i] < largest] or [i for i in range(1, amount) if counts[i] < bound]
        mass, left = sum([portions[i] for i in free]), spare
        for i in free:
            addition = min(bound - counts[i], max(1, left * portions[i] // mass), spare)
            counts[i] = counts[i] + addition
            spare = spare - addition
    return np.array(counts)


def gaussian(rng, shape, deviation, reach, shards=(), held_as=jnp.bfloat16):
    entries = jax.random.normal(rng, shape, jnp.float32) * deviation
    if len(shards) > 0:
        entries = steps_of(rng, shape, shards, -0.22, 0.18) * entries
    return jnp.clip(entries, min=-reach, max=reach).astype(held_as)


def setup_inputs(seed: int = 0) -> dict:
    streams_of = jax.random.split(jax.random.key(seed), 20)
    resid = gaussian(streams_of[0], (TOKENS, D), 1.0, 6.0, ((0, 32),))
    query_one = draw_query_one(jax.random.fold_in(streams_of[19], 71), 0)
    query_two = draw_query_two(jax.random.fold_in(streams_of[19], 71), 0)
    key_one = draw_key_one(jax.random.fold_in(streams_of[19], 71), 0)
    key_two = draw_key_two(jax.random.fold_in(streams_of[19], 71), 0)
    values = gaussian(streams_of[5], (TOKENS, HEADS * VAL_DIM), 1.0, 6.0, ((0, 32), (1, 8)))
    documents = jnp.searchsorted(jnp.cumsum(ragged(streams_of[6], DOC_COUNT, TOKENS, DOC_MOST, 0)), jnp.arange(TOKENS), side="right").astype(jnp.int32)
    mix_lambda = jnp.clip(0.3 + 0.5 * jax.random.uniform(streams_of[7], (HEADS,), jnp.float32) ** steps_of(streams_of[7], (HEADS,), ((0, 8),), -0.2, 0.2), 0.3, 0.8)
    head_gain = jnp.clip(1.0 + 0.18 * jax.random.normal(streams_of[8], (VAL_DIM,), jnp.float32), 0.1, 1.9)
    out_weight = gaussian(streams_of[9], (HEADS * VAL_DIM, D), (HEADS * VAL_DIM) ** -0.5, 0.125, ((0, 8),))
    ffn_gain = jnp.clip(1.0 + 0.18 * jax.random.normal(streams_of[10], (D,), jnp.float32), 0.1, 1.9)
    routes_keys = jax.random.split(jax.random.fold_in(streams_of[11], 1), TOKENS // TOK_DEV)
    routes_turns = jax.random.permutation(jax.random.fold_in(streams_of[11], 3), TOKENS // TOK_DEV)
    routes = jax.vmap(lambda own, number: deal_out(jax.random.fold_in(streams_of[11], 2), own, number, TOK_DEV, EXPERTS, TOP, CAP, 2))(routes_keys, routes_turns).reshape((TOKENS, TOP))
    route_weight = jnp.clip(0.2 + 0.7 * jax.random.uniform(streams_of[12], (TOKENS, TOP), jnp.float32) ** steps_of(streams_of[12], (TOKENS, TOP), ((0, 32),), -0.2, 0.2), 0.2, 0.9)
    expert_gate = gaussian(streams_of[13], (EXPERTS, D, EXP_FF), D ** -0.5, 0.125, ((0, 256),))
    expert_up = gaussian(streams_of[14], (EXPERTS, D, EXP_FF), D ** -0.5, 0.125, ((0, 256),))
    expert_down = gaussian(streams_of[15], (EXPERTS, EXP_FF, D), EXP_FF ** -0.5, 0.25, ((0, 256),))
    shared_gate = gaussian(streams_of[16], (D, SHARED_FF), D ** -0.5, 0.125, ((1, 8),))
    shared_up = gaussian(streams_of[17], (D, SHARED_FF), D ** -0.5, 0.125, ((1, 8),))
    shared_down = gaussian(streams_of[18], (SHARED_FF, D), SHARED_FF ** -0.5, 0.25, ((0, 8),))
    return dict(resid=resid, query_one=query_one, query_two=query_two, key_one=key_one, key_two=key_two, values=values, documents=documents, mix_lambda=mix_lambda, head_gain=head_gain, out_weight=out_weight, ffn_gain=ffn_gain, routes=routes, route_weight=route_weight, expert_gate=expert_gate, expert_up=expert_up, expert_down=expert_down, shared_gate=shared_gate, shared_up=shared_up, shared_down=shared_down)


HEAD_SCALE = 0.8

def head_rows(inputs, documents, head_gain):
    query_first, query_second, key_first, key_second, value_rows, lambda_value = inputs
    seq_len = key_first.shape[0]
    key_pos = jnp.arange(seq_len, dtype=jnp.int32)
    score_scale = HEAD_DIM ** (-0.5)

    def query_block(block_idx):
        offset = block_idx * TOK_DEV
        query_pos = offset + jnp.arange(TOK_DEV, dtype=jnp.int32)
        query_docs = lax.dynamic_slice_in_dim(documents, offset, TOK_DEV, 0)
        allowed = (key_pos[None, :] <= query_pos[:, None]) & (documents[None, :] == query_docs[:, None])

        def probs(queries, keys):
            block_query = lax.dynamic_slice_in_dim(queries, offset, TOK_DEV, 0)
            raw = jnp.dot(block_query, keys.T, preferred_element_type=jnp.float32) * score_scale
            masked = jnp.where(allowed, raw, -jnp.inf)
            top_row = lax.optimization_barrier(jnp.max(masked, axis=-1, keepdims=True))
            exp_terms = jnp.where(allowed, jnp.exp(masked - top_row), 0.0)
            return exp_terms / lax.optimization_barrier(jnp.sum(exp_terms, axis=-1, keepdims=True))
        weights = (probs(query_first, key_first) - lambda_value * probs(query_second, key_second)).astype(jnp.bfloat16)
        return jnp.dot(weights, value_rows, preferred_element_type=jnp.float32)
    blocks = lax.map(query_block, jnp.arange(seq_len // TOK_DEV, dtype=jnp.int32))
    head_out = blocks.reshape(seq_len, VAL_DIM)
    scaled = head_out * lax.rsqrt(lax.optimization_barrier(jnp.mean(head_out * head_out, axis=-1, keepdims=True)) + 1e-05)
    return (scaled * head_gain * HEAD_SCALE).astype(jnp.bfloat16)

def by_head(array_in, width):
    return array_in.reshape(TOKENS, HEADS, width).transpose(1, 0, 2)

def reference(resid, query_one, query_two, key_one, key_two, values, documents, mix_lambda, head_gain, out_weight, ffn_gain, routes, route_weight, expert_gate, expert_up, expert_down, shared_gate, shared_up, shared_down):
    head_fn = partial(head_rows, documents=documents, head_gain=head_gain)
    heads_out = lax.map(head_fn, (by_head(query_one, HEAD_DIM), by_head(query_two, HEAD_DIM), by_head(key_one, HEAD_DIM), by_head(key_two, HEAD_DIM), by_head(values, VAL_DIM), mix_lambda))
    attn_rows = heads_out.transpose(1, 0, 2).reshape(TOKENS, HEADS * VAL_DIM)
    group_cols = HEADS // N_TP * VAL_DIM
    projected = jnp.zeros((TOKENS, D), jnp.float32)
    for group in range(N_TP):
        part_sum = jnp.dot(attn_rows[:, group * group_cols:(group + 1) * group_cols], out_weight[group * group_cols:(group + 1) * group_cols], preferred_element_type=jnp.float32)
        projected = projected + lax.optimization_barrier(part_sum.astype(jnp.bfloat16)).astype(jnp.float32)
    mixed = resid.astype(jnp.float32) + projected
    normed = (mixed * lax.rsqrt(lax.optimization_barrier(jnp.mean(mixed * mixed, axis=-1, keepdims=True)) + 1e-06) * ffn_gain).astype(jnp.bfloat16)
    assign_total = TOKENS * TOP
    flat_expert = routes.reshape(assign_total)
    flat_weight = route_weight.reshape(assign_total)
    assign_token = jnp.arange(assign_total, dtype=jnp.int32) // TOP
    assign_block = jnp.arange(assign_total, dtype=jnp.int32) // (TOK_DEV * TOP)
    one_hot = (flat_expert[:, None] == jnp.arange(EXPERTS, dtype=jnp.int32)[None, :]).astype(jnp.int32)
    running = jnp.cumsum(one_hot.reshape(N_SP, TOK_DEV * TOP, EXPERTS), axis=1).reshape(assign_total, EXPERTS)
    slot_rank = lax.optimization_barrier(jnp.sum(running * one_hot, axis=1)) - 1
    slot_id = (flat_expert * (N_SP * CAP) + assign_block * CAP + slot_rank).astype(jnp.int32)
    slot_token = jnp.full((EXPERTS * N_SP * CAP,), TOKENS, jnp.int32).at[slot_id].set(assign_token)
    padded = jnp.concatenate([normed, jnp.zeros((1, D), jnp.bfloat16)], axis=0)

    def run_expert(inputs):
        token_idx, gate_w, up_w, down_w = inputs
        rows_in = padded[token_idx]
        gate_part = jnp.dot(rows_in, gate_w, preferred_element_type=jnp.float32)
        up_part = jnp.dot(rows_in, up_w, preferred_element_type=jnp.float32)
        hidden = (jax.nn.silu(gate_part) * up_part).astype(jnp.bfloat16)
        return jnp.dot(hidden, down_w, preferred_element_type=jnp.float32).astype(jnp.bfloat16)
    expert_rows = lax.map(run_expert, (slot_token.reshape(EXPERTS, N_SP * CAP), expert_gate, expert_up, expert_down))
    flat_rows = expert_rows.reshape(EXPERTS * N_SP * CAP, D)
    weighted = (flat_rows[slot_id].astype(jnp.float32) * flat_weight[:, None]).reshape(TOKENS, TOP, D)
    expert_group = routes % N_TP
    shared_act = (jax.nn.silu(jnp.dot(normed, shared_gate, preferred_element_type=jnp.float32)) * jnp.dot(normed, shared_up, preferred_element_type=jnp.float32)).astype(jnp.bfloat16)
    shared_cols = SHARED_FF // N_TP
    ffn_total = jnp.zeros((TOKENS, D), jnp.float32)
    for group in range(N_TP):
        chosen = (expert_group == group).astype(jnp.float32)
        routed = lax.optimization_barrier(jnp.sum(weighted * chosen[:, :, None], axis=1))
        shared_part = jnp.dot(shared_act[:, group * shared_cols:(group + 1) * shared_cols], shared_down[group * shared_cols:(group + 1) * shared_cols], preferred_element_type=jnp.float32)
        ffn_total = ffn_total + lax.optimization_barrier((routed + shared_part).astype(jnp.bfloat16)).astype(jnp.float32)
    return (mixed + ffn_total).astype(jnp.bfloat16)
```

```python
from functools import partial

import jax
import jax.numpy as jnp
from jax import lax
from jax.experimental import pallas as pl
from jax.experimental.pallas import tpu as pltpu
from jax.sharding import Mesh, PartitionSpec as P


NEG_FILL = -1e30
HEAD_SCALE = 0.8
NZ, NX, NY, NC = 8, 4, 4, 2
TOK = 256
D = 2048
HALF = 128
CAP = 8
SLOTS = NZ * NX * CAP
LOG2E = 1.4426950408889634
BF = jnp.bfloat16
F32 = jnp.float32
SMEM = pl.BlockSpec(memory_space=pltpu.SMEM)
VMEM = pl.BlockSpec(memory_space=pltpu.VMEM)
VLIM = 48 * 1024 * 1024


def shift(value, axis, step):
    size = lax.axis_size(axis)
    return lax.ppermute(value, axis, [(i, (i + step) % size) for i in range(size)])


def swap(value):
    return shift(value, "c", 1)


def call(kernel, scalars, operands, outs, scratch=(), flops=0, name=None):
    return pl.pallas_call(
        kernel,
        out_shape=outs,
        in_specs=[SMEM] * len(scalars) + [VMEM] * len(operands),
        out_specs=jax.tree.map(lambda _: VMEM, outs),
        scratch_shapes=list(scratch),
        compiler_params=pltpu.CompilerParams(vmem_limit_bytes=VLIM),
        cost_estimate=pl.CostEstimate(flops=flops, bytes_accessed=0, transcendentals=0),
        name=name,
    )(*scalars, *operands)


def iota(shape, dim):
    return lax.broadcasted_iota(jnp.int32, shape, dim)


def pack_kernel(pos, q1, q2, k1, k2, v, *outs):
    x = pos[1]
    row = iota((128, 128), 0)
    col = iota((128, 128), 1)
    for turn, out in enumerate(outs):
        index = x ^ turn
        head = index >> 1
        core = index & 1
        first = ((col < 64) & (row == col + 64 * head)).astype(BF)
        second = ((col >= 64) & (row == col - 64 + 64 * head)).astype(BF)

        def rows(ref, lanes):
            return jnp.concatenate(
                [
                    ref[pl.ds(pl.multiple_of(64 * i + 32 * core, 32), 32), lanes]
                    for i in range(4)
                ],
                axis=0,
            )

        every = slice(None)

        def merged(a, b):
            return (
                jnp.dot(rows(a, every), first, preferred_element_type=F32)
                + jnp.dot(rows(b, every), second, preferred_element_type=F32)
            ).astype(BF)

        out[:, 0:128] = merged(q1, q2)
        out[:, 128:256] = merged(k1, k2)
        out[:, 256:384] = rows(v, pl.ds(pl.multiple_of(128 * head, 128), 128))


def unpack_kernel(pos, r0, r1, r2, r3, low, high, queries):
    mine = (pos[1] & 1) * 2 + pos[3]
    lane = iota((HALF, 128), 1)
    for turn, ref in enumerate((r0, r1, r2, r3)):
        block = mine ^ turn

        @pl.when(block < 2)
        def _():
            low[block] = ref[:, 128:384]

        @pl.when(block >= 2)
        def _():
            high[block - 2] = ref[:, 128:384]

        both = ref[:, 0:128]
        start = pl.multiple_of(block * HALF, HALF)
        queries[pl.ds(start, HALF), :] = jnp.where(lane < 64, both, jnp.zeros_like(both))
        queries[pl.ds(start + 512, HALF), :] = jnp.where(lane < 64, jnp.zeros_like(both), both)


ROWS = 256


def attend_kernel(kinds, first_call, last_call, pos, *refs):
    refs = list(refs)
    queries, starts = refs[0], refs[1]
    at = 2
    if last_call:
        lam, gain = refs[at], refs[at + 1]
        at += 2
    if not first_call:
        state_in = refs[at : at + 3]
        at += 3
    planes = []
    for back, blocks in kinds:
        count = 2 if blocks == 1 else 4
        planes.append((back, blocks, refs[at : at + count]))
        at += count
    if last_call:
        out = refs[at]
        tops, sums, acc = refs[at + 1 : at + 4]
    else:
        tops, sums, acc = refs[at : at + 3]
    z, core, least = pos[0], pos[3], pos[4]

    def setup(tile):
        rows = pl.ds(pl.multiple_of(tile * ROWS, ROWS), ROWS)
        if first_call:
            tops[rows, :] = jnp.full((ROWS, 128), NEG_FILL, F32)
            sums[rows, :] = jnp.zeros((ROWS, 128), F32)
            acc[rows, :] = jnp.zeros((ROWS, 128), F32)
        else:
            for dst, src in zip((tops, sums, acc), state_in):
                dst[rows, :] = src[rows, :]

    def step(tile, back, blocks, arrays):
        rows = pl.ds(pl.multiple_of(tile * ROWS, ROWS), ROWS)
        count = blocks * TOK
        if blocks == 1:
            parts = [arrays[0][...], arrays[1][...]]
        else:
            parts = []
            for b in range(4):
                parts += [arrays[b // 2][b % 2], arrays[2 + b // 2][b % 2]]
        keys = jnp.concatenate([p[:, 0:128] for p in parts], axis=0)
        vals = jnp.concatenate([p[:, 128:256] for p in parts], axis=0)
        raw = lax.dot_general(
            queries[rows, :], keys, (((1,), (1,)), ((), ())), preferred_element_type=F32
        )
        scaled = raw * (0.125 * LOG2E)
        at_key = iota((1, count), 1)
        lane = at_key & 127
        base = (z - back) * (4 * TOK) + (4 - blocks) * TOK
        key_pos = (
            base
            + (at_key >> 8) * TOK
            + 64 * (lane >> 5)
            + 32 * (core ^ ((at_key >> 7) & 1))
            + (lane & 31)
        )
        allowed = key_pos >= starts[rows, :]
        if back == 0:
            at_row = (iota((ROWS, 1), 0) + tile * ROWS) & 511
            row = at_row & 127
            query_pos = (
                z * (4 * TOK) + (at_row >> 7) * TOK + 64 * (row >> 5) + 32 * core + (row & 31)
            )
            allowed = allowed & (key_pos <= query_pos)
        masked = jnp.where(allowed, scaled, NEG_FILL)
        old = tops[rows, :][:, 0:1]
        new = jnp.maximum(old, jnp.max(masked, axis=1, keepdims=True))
        probs = jnp.exp2(masked - new)
        fade = jnp.exp2(old - new)
        tops[rows, :] = jnp.broadcast_to(new, (ROWS, 128))
        sums[rows, :] = sums[rows, :] * fade + jnp.sum(probs, axis=1, keepdims=True)
        acc[rows, :] = acc[rows, :] * fade + jnp.dot(
            probs.astype(BF), vals, preferred_element_type=F32
        )

    def over_tiles(body):
        def turn(tile, carry):
            body(tile)
            return carry

        lax.fori_loop(0, 1024 // ROWS, turn, 0)

    over_tiles(setup)
    for back, blocks, arrays in planes:
        if back == 0:
            over_tiles(lambda tile: step(tile, back, blocks, arrays))
        else:

            @pl.when((z >= back) & ((z - back + 1) * (4 * TOK) > least))
            def _():
                over_tiles(lambda tile: step(tile, back, blocks, arrays))

    if last_call:
        one = acc[0:512, :] / sums[0:512, :]
        two = acc[512:1024, :] / sums[512:1024, :]
        head = one - lam[...] * two
        scale = lax.rsqrt(jnp.mean(head * head, axis=1, keepdims=True) + 1e-5)
        out[...] = (head * scale * gain[...] * HEAD_SCALE).astype(BF)


def attend(pos, queries, starts, planes, state=None, finish=None):
    kinds = tuple((back, blocks) for back, blocks, _ in planes)
    operands = [queries, starts]
    if finish is not None:
        operands += list(finish)
    if state is not None:
        operands += list(state)
    for _, _, arrays in planes:
        operands += list(arrays)
    big = jax.ShapeDtypeStruct((1024, 128), F32)
    kernel = partial(attend_kernel, kinds, state is None, finish is not None)
    keys = sum(blocks * TOK for _, blocks in kinds)
    if finish is not None:
        outs = jax.ShapeDtypeStruct((512, 128), BF)
        scratch = [pltpu.VMEM((1024, 128), F32)] * 3
    else:
        outs = (big, big, big)
        scratch = []
    return call(
        kernel, [pos], operands, outs, scratch, flops=1024 * keys * 512, name="attend"
    )


def project_kernel(pos, attn, resid, gain, *refs):
    weights, (mixed, normed) = refs[:-2], refs[-2:]
    y, core = pos[2], pos[3]
    total = resid[...].astype(F32)
    order = []
    for flip in range(2):
        w = weights[5 * flip : 5 * flip + 5]
        order += [(w[0], 0, flip, 0, 256), (w[1], 3, flip, 0, 256), (w[2], 1, flip, 0, 256)]
        order += [(w[3], 2, flip, 0, 128), (w[4], 2, flip, 128, 128)]
    for w, ahead, flip, low, size in order:
        src = (y + ahead) & 3
        head = 2 * (core ^ flip)
        pieces = []
        for part in range(low // 128, (low + size) // 128):
            pieces.append(attn[(head + part) * 4 + src])
        lhs = pieces[0] if len(pieces) == 1 else jnp.concatenate(pieces, axis=1)
        total = total + jnp.dot(lhs, w[...], preferred_element_type=F32)
    mixed[...] = total
    scale = lax.rsqrt(jnp.mean(total * total, axis=1, keepdims=True) + 1e-6)
    normed[...] = (total * scale * gain[...]).astype(BF)


def route_kernel(pos, routes, weights, pick, high, low):
    group = pos[2] * NC + pos[3]
    target = iota((NZ * NX, TOK), 0) * (NY * NC) + group
    hits = jnp.zeros((NZ * NX, TOK), F32)
    gains = jnp.zeros((NZ * NX, TOK), F32)
    for k in range(4):
        same = routes[k : k + 1, :] == target
        hits = hits + jnp.where(same, 1.0, 0.0)
        gains = gains + jnp.where(same, weights[k : k + 1, :], 0.0)
    before = (iota((TOK, TOK), 0) < iota((TOK, TOK), 1)).astype(BF)
    rank = jnp.dot(hits.astype(BF), before, preferred_element_type=F32)
    rank = jnp.where(hits > 0.5, rank, -1.0)
    slot = iota((NZ * NX, CAP, TOK), 1).astype(F32)
    chosen = (jnp.broadcast_to(rank[:, None, :], (NZ * NX, CAP, TOK)) == slot).reshape(SLOTS, TOK)
    spread = jnp.broadcast_to(gains[:, None, :], (NZ * NX, CAP, TOK)).reshape(SLOTS, TOK)
    pick[...] = jnp.where(chosen, 1.0, 0.0).astype(BF)
    full = jnp.where(chosen, spread, 0.0).T
    upper = full.astype(BF)
    high[...] = upper
    low[...] = (full - upper.astype(F32)).astype(BF)


def dispatch_kernel(pos, pick, *refs):
    chunks, (outgoing, rows) = refs[:-2], refs[-2:]
    y = pos[2]
    for flip in range(2):
        for ahead, ref in zip((0, 3, 1, 2), chunks[4 * flip : 4 * flip + 4]):
            src = (y + ahead) & 3
            rows[pl.ds(pl.multiple_of(flip * HALF + src * 32, 32), 32), :] = ref[...]
    outgoing[...] = jnp.dot(pick[...], rows[...], preferred_element_type=F32).astype(BF)


def shared_kernel(rows, gate, up, down, out):
    gated = jnp.dot(rows[...], gate[...], preferred_element_type=F32)
    lifted = jnp.dot(rows[...], up[...], preferred_element_type=F32)
    act = (gated / (1.0 + jnp.exp(-gated)) * lifted).astype(BF)
    out[...] = jnp.dot(act, down[...], preferred_element_type=F32)


def expert_kernel(rows, gate, up, down, out):
    gated = jnp.dot(rows[...], gate[...], preferred_element_type=F32)
    lifted = jnp.dot(rows[...], up[...], preferred_element_type=F32)
    act = (gated / (1.0 + jnp.exp(-gated)) * lifted).astype(BF)
    out[...] = jnp.dot(act, down[...], preferred_element_type=F32).astype(BF)


def combine_kernel(high, low, rows, shared, keep, send):
    total = (
        jnp.dot(high[...], rows[...], preferred_element_type=F32)
        + jnp.dot(low[...], rows[...], preferred_element_type=F32)
        + shared[...]
    ).astype(BF)
    keep[...] = total[:HALF]
    send[...] = total[HALF:]


def local(
    resid,
    query_one,
    query_two,
    key_one,
    key_two,
    values,
    documents,
    mix_lambda,
    head_gain,
    out_weight,
    ffn_gain,
    routes,
    route_weight,
    expert_gate,
    expert_up,
    expert_down,
    shared_gate,
    shared_up,
    shared_down,
):
    iz, ix, iy, ic = (lax.axis_index(a) for a in ("z", "x", "y", "c"))
    pos = jnp.stack([iz, ix, iy, ic, jnp.int32(0)])
    plane_axes = ("z", "x")

    copies = jnp.broadcast_to(documents[None, None, :], (NZ * NX, 1, TOK))
    docs = lax.all_to_all(copies, plane_axes, split_axis=0, concat_axis=0, tiled=True)

    packed = call(
        pack_kernel,
        [pos],
        [query_one, query_two, key_one, key_two, values],
        tuple(jax.ShapeDtypeStruct((HALF, 384), BF) for _ in range(4)),
        name="pack",
    )

    def turn_pairs(turn):
        pairs = []
        for x in range(NX):
            for c in range(NC):
                index = x ^ turn
                pairs.append((x * NC + c, (2 * c + (index >> 1)) * NC + (index & 1)))
        return pairs

    came = [lax.ppermute(packed[t], ("x", "c"), turn_pairs(t)) for t in range(4)]
    half = jax.ShapeDtypeStruct((2, HALF, 256), BF)
    low0, high0, queries = call(
        unpack_kernel,
        [pos],
        came,
        (half, half, jax.ShapeDtypeStruct((1024, 128), BF)),
        name="unpack",
    )
    lambda_pair = swap(mix_lambda[None, :])[0]
    lambdas = jnp.where(ic == 0, jnp.concatenate([mix_lambda, lambda_pair]), jnp.concatenate([lambda_pair, mix_lambda]))
    lam = lax.dynamic_slice_in_dim(lambdas, ix, 1, 0).reshape(1, 1)

    low1, high1 = shift(low0, "z", 1), shift(high0, "z", 1)
    back2 = shift(high0, "z", -2)
    back3 = shift(high0[1], "z", -3)
    low2, high2 = shift(low1, "z", 1), shift(high1, "z", 1)
    high4 = shift(back2, "z", -2)
    low3, high3 = shift(low2, "z", 1), shift(high2, "z", 1)
    low4 = shift(low3, "z", 1)

    def plane(low, high):
        return [low, high, swap(low), swap(high)]

    flat = docs.reshape(NZ * NX * TOK)
    own_docs = lax.dynamic_slice_in_dim(docs.reshape(NZ, NX, 4, NC, 32), iz, 1, 0)[0]
    own_docs = lax.dynamic_slice_in_dim(own_docs, ic, 1, 2).reshape(512)
    counts = [jnp.sum((flat < d).astype(jnp.int32)) for d in range(8)]
    starts = sum(jnp.where(own_docs == d, counts[d], 0) for d in range(8))
    least = jnp.min(starts)
    pos_attn = jnp.stack([iz, ix, iy, ic, least])
    starts = jnp.concatenate([starts, starts]).reshape(1024, 1)

    state = attend(pos_attn, queries, starts, [(0, 4, plane(low0, high0))])
    state = attend(pos_attn, queries, starts, [(1, 4, plane(low1, high1))], state)
    state = attend(
        pos_attn,
        queries,
        starts,
        [(2, 4, plane(low2, high2)), (5, 1, [back3, swap(back3)])],
        state,
    )
    heads = attend(
        pos_attn,
        queries,
        starts,
        [(3, 4, plane(low3, high3)), (4, 4, plane(low4, high4))],
        state,
        finish=(lam, head_gain.reshape(1, 128)),
    )

    from_left = shift(out_weight, "y", 1)
    from_right = shift(out_weight, "y", -1)
    far_a = shift(from_left[:HALF], "y", 1)
    far_b = shift(from_right[HALF:], "y", -1)
    mine = [out_weight, from_left, from_right, far_a, far_b]
    full_weight = mine + [swap(w) for w in mine]

    attn = lax.all_to_all(
        heads.reshape(NX * NY, 32, 128), ("x", "y"), split_axis=0, concat_axis=0, tiled=True
    )
    own_start = (iy * NC + ic) * 32
    resid_own = lax.dynamic_slice_in_dim(resid, own_start, 32, 0)
    mixed, normed = call(
        project_kernel,
        [pos],
        [attn, resid_own, ffn_gain.reshape(1, D)] + full_weight,
        (
            jax.ShapeDtypeStruct((32, D), F32),
            jax.ShapeDtypeStruct((32, D), BF),
        ),
        flops=2 * 32 * D * D,
        name="project",
    )

    chunks = [normed, shift(normed, "y", 1), shift(normed, "y", -1), shift(normed, "y", 2)]
    chunks = chunks + [swap(c) for c in chunks]

    def ordered(table):
        parts = table.T.reshape(4, NY, NC, 32)
        own = lax.dynamic_slice_in_dim(parts, ic, 1, 2)[:, :, 0]
        other = lax.dynamic_slice_in_dim(parts, 1 - ic, 1, 2)[:, :, 0]
        return jnp.concatenate([own.reshape(4, HALF), other.reshape(4, HALF)], axis=1)

    table = jax.ShapeDtypeStruct((SLOTS, TOK), BF)
    pick, weight_high, weight_low = call(
        route_kernel,
        [pos],
        [ordered(routes), ordered(route_weight)],
        (table, jax.ShapeDtypeStruct((TOK, SLOTS), BF), jax.ShapeDtypeStruct((TOK, SLOTS), BF)),
        name="route",
    )
    outgoing, rows = call(
        dispatch_kernel,
        [pos],
        [pick] + chunks,
        (jax.ShapeDtypeStruct((SLOTS, D), BF), jax.ShapeDtypeStruct((TOK, D), BF)),
        flops=2 * SLOTS * TOK * D,
        name="dispatch",
    )
    arrived = lax.all_to_all(
        outgoing.reshape(NZ * NX, CAP, D), plane_axes, split_axis=0, concat_axis=0, tiled=True
    )
    shared = call(
        shared_kernel,
        [],
        [rows, shared_gate, shared_up, shared_down],
        jax.ShapeDtypeStruct((TOK, D), F32),
        flops=2 * TOK * D * 192,
        name="shared",
    )
    result = call(
        expert_kernel,
        [],
        [arrived.reshape(SLOTS, D), expert_gate[0], expert_up[0], expert_down[0]],
        jax.ShapeDtypeStruct((SLOTS, D), BF),
        flops=2 * SLOTS * D * 1536,
        name="expert",
    )
    returned = lax.all_to_all(
        result.reshape(NZ * NX, CAP, D), plane_axes, split_axis=0, concat_axis=0, tiled=True
    ).reshape(SLOTS, D)
    part = jax.ShapeDtypeStruct((HALF, D), BF)
    keep, send = call(
        combine_kernel,
        [],
        [weight_high, weight_low, returned, shared],
        (part, part),
        flops=4 * SLOTS * TOK * D,
        name="combine",
    )
    pair_sum = (keep.astype(F32) + swap(send).astype(F32)).astype(BF)
    ffn = lax.all_to_all(
        pair_sum.reshape(NY, 32, D), "y", split_axis=0, concat_axis=0, tiled=True
    )
    return (mixed + ffn.astype(F32).sum(axis=0)).astype(BF)


def solution(mesh):
    split = Mesh(mesh.devices.reshape(NZ, NX, NY, NC), ("z", "x", "y", "c"))
    sp, tp, both = ("z", "x"), ("y", "c"), ("z", "x", "y", "c")
    placed = (
        P(sp, None),
        P(sp, tp),
        P(sp, tp),
        P(sp, tp),
        P(sp, tp),
        P(sp, tp),
        P(sp),
        P(tp),
        P(),
        P(tp, None),
        P(),
        P(sp, None),
        P(sp, None),
        P(both, None, None),
        P(both, None, None),
        P(both, None, None),
        P(None, tp),
        P(None, tp),
        P(tp, None),
    )
    return jax.shard_map(
        local, mesh=split, in_specs=placed, out_specs=P(both, None), check_vma=False
    )
```

```python
from functools import partial

import jax
import jax.numpy as jnp
from jax import lax
from jax.experimental import pallas as pl
from jax.experimental.pallas import tpu as pltpu
from jax.sharding import Mesh, PartitionSpec as P


NEG_FILL = -1e30
HEAD_SCALE = 0.8
NZ, NX, NY, NC = 8, 4, 4, 2
TOK = 256
D = 2048
HALF = 128
CAP = 8
SLOTS = NZ * NX * CAP
LOG2E = 1.4426950408889634
BF = jnp.bfloat16
F32 = jnp.float32
SMEM = pl.BlockSpec(memory_space=pltpu.SMEM)
VMEM = pl.BlockSpec(memory_space=pltpu.VMEM)
VLIM = 28 * 1024 * 1024


def shift(value, axis, step):
    size = lax.axis_size(axis)
    return lax.ppermute(value, axis, [(i, (i + step) % size) for i in range(size)])


def swap(value):
    return shift(value, "c", 1)


def after(value, *others):
    return lax.optimization_barrier((value, *others))[0]


def call(kernel, scalars, operands, outs, scratch=(), flops=0):
    return pl.pallas_call(
        kernel,
        out_shape=outs,
        in_specs=[SMEM] * len(scalars) + [VMEM] * len(operands),
        out_specs=jax.tree.map(lambda _: VMEM, outs),
        scratch_shapes=list(scratch),
        compiler_params=pltpu.CompilerParams(vmem_limit_bytes=VLIM),
        cost_estimate=pl.CostEstimate(flops=flops, bytes_accessed=0, transcendentals=0),
    )(*scalars, *operands)


def iota(shape, dim):
    return lax.broadcasted_iota(jnp.int32, shape, dim)


LINES = HALF + 8


def pack_kernel(pos, lam, docs, q1, q2, k1, k2, v, *rest):
    outs, (q1v, q2v, k1v, k2v, vv, sems) = rest[:4], rest[4:]
    pairs = ((q1, q1v), (q2, q2v), (k1, k1v), (k2, k2v), (v, vv))
    loads = [pltpu.make_async_copy(a, b, sems.at[i]) for i, (a, b) in enumerate(pairs)]
    for load in loads:
        load.start()
    x = pos[1]
    row = iota((128, 128), 0)
    col = iota((128, 128), 1)
    place = iota((TOK, 128), 0)
    lane = iota((TOK, 128), 1)
    line = iota((8, 128), 0)
    numbers = jnp.broadcast_to(docs[...].astype(F32), (8, TOK)).astype(BF)
    for load in loads:
        load.wait()
    for turn, out in enumerate(outs):
        index = x ^ turn
        head = index >> 1
        core = index & 1
        first = ((col < 64) & (row == col + 64 * head)).astype(BF)
        second = ((col >= 64) & (row == col - 64 + 64 * head)).astype(BF)

        def rows(ref, lanes):
            return jnp.concatenate(
                [
                    ref[pl.ds(pl.multiple_of(64 * i + 32 * core, 32), 32), lanes]
                    for i in range(4)
                ],
                axis=0,
            )

        every = slice(None)

        def merged(a, b):
            return (
                jnp.dot(rows(a, every), first, preferred_element_type=F32)
                + jnp.dot(rows(b, every), second, preferred_element_type=F32)
            ).astype(BF)

        out[0:HALF, 0:128] = merged(q1v, q2v)
        out[0:HALF, 128:256] = merged(k1v, k2v)
        out[0:HALF, 256:384] = rows(vv, pl.ds(pl.multiple_of(128 * head, 128), 128))
        taken = (place == 64 * (lane >> 5) + 32 * core + (lane & 31)).astype(BF)
        own_docs = jnp.dot(numbers, taken, preferred_element_type=F32)
        mixing = jnp.where(head == 0, lam[0], lam[1])
        mixing = jnp.full((8, 128), mixing, F32)
        upper = mixing.astype(BF).astype(F32)
        middle = (mixing - upper).astype(BF).astype(F32)
        lower = mixing - upper - middle
        extra = jnp.where(
            line == 0,
            own_docs,
            jnp.where(line == 1, upper, jnp.where(line == 2, middle, lower)),
        ).astype(BF)
        out[HALF:LINES, 0:128] = extra
        out[HALF:LINES, 128:256] = extra
        out[HALF:LINES, 256:384] = extra


def unpack_kernel(pos, r0, r1, r2, r3, keys, edge, queries, docs, lam):
    mine = (pos[1] & 1) * 2 + pos[3]
    lane = iota((HALF, 128), 1)
    unit = (iota((HALF, 128), 0) == lane).astype(BF)
    for turn, ref in enumerate((r0, r1, r2, r3)):
        block = mine ^ turn
        keys[block] = ref[:, 128:384]

        @pl.when(block == NX - 1)
        def _():
            edge[...] = ref[:, 128:384]

        both = ref[0:HALF, 0:128]
        start = pl.multiple_of(block * HALF, HALF)
        queries[pl.ds(start, HALF), :] = jnp.where(lane < 64, both, jnp.zeros_like(both))
        queries[pl.ds(start + 512, HALF), :] = jnp.where(lane < 64, jnp.zeros_like(both), both)
        extra = ref[HALF:LINES, 0:128].astype(F32)
        spread = jnp.broadcast_to(extra[0:1, :], (HALF, 128)).astype(BF)
        column = lax.dot_general(
            unit, spread, (((1,), (1,)), ((), ())), preferred_element_type=F32
        )
        docs[pl.ds(start, HALF), :] = column
        docs[pl.ds(start + 512, HALF), :] = column
        if turn == 0:
            total = extra[1:2, :] + extra[2:3, :] + extra[3:4, :]
            lam[...] = jnp.broadcast_to(total, (8, 128))


ROWS = 256


def attend_kernel(kinds, first_call, last_call, pos, *refs):
    refs = list(refs)
    queries, query_docs = refs[0], refs[1]
    at = 2
    if last_call:
        lam, gain = refs[at], refs[at + 1]
        at += 2
    if not first_call:
        state_in = refs[at : at + 3]
        at += 3
    planes = []
    for back, blocks in kinds:
        count = 2
        planes.append((back, blocks, refs[at : at + count]))
        at += count
    if last_call:
        out = refs[at]
        tops, sums, acc = refs[at + 1 : at + 4]
    else:
        tops, sums, acc = refs[at : at + 3]
    z, core = pos[0], pos[3]
    least = jnp.min(query_docs[0:8, :])

    def setup(tile):
        rows = pl.ds(pl.multiple_of(tile * ROWS, ROWS), ROWS)
        if first_call:
            tops[rows, :] = jnp.full((ROWS, 128), NEG_FILL, F32)
            sums[rows, :] = jnp.zeros((ROWS, 128), F32)
            acc[rows, :] = jnp.zeros((ROWS, 128), F32)
        else:
            for dst, src in zip((tops, sums, acc), state_in):
                dst[rows, :] = src[rows, :]

    def step(tile, back, blocks, arrays):
        rows = pl.ds(pl.multiple_of(tile * ROWS, ROWS), ROWS)
        count = blocks * TOK
        parts = [
            ref[:, :] if blocks == 1 else ref[b] for b in range(blocks) for ref in arrays
        ]
        numbers = jnp.concatenate([p[HALF:LINES, 0:128].astype(F32) for p in parts], axis=1)
        key_docs = numbers[0:1, :]
        parts = [p[0:HALF] for p in parts]
        keys = jnp.concatenate([p[:, 0:128] for p in parts], axis=0)
        vals = jnp.concatenate([p[:, 128:256] for p in parts], axis=0)
        raw = lax.dot_general(
            queries[rows, :], keys, (((1,), (1,)), ((), ())), preferred_element_type=F32
        )
        scaled = raw * (0.125 * LOG2E)
        allowed = key_docs == query_docs[rows, :][:, 0:1]
        if back == 0:
            at_key = iota((1, count), 1)
            lane = at_key & 127
            key_pos = (
                (at_key >> 8) * TOK
                + 64 * (lane >> 5)
                + 32 * (core ^ ((at_key >> 7) & 1))
                + (lane & 31)
            )
            at_row = (iota((ROWS, 1), 0) + tile * ROWS) & 511
            row = at_row & 127
            query_pos = (at_row >> 7) * TOK + 64 * (row >> 5) + 32 * core + (row & 31)
            allowed = allowed & (key_pos <= query_pos)
        masked = jnp.where(allowed, scaled, NEG_FILL)
        old = tops[rows, :][:, 0:1]
        new = jnp.maximum(old, jnp.max(masked, axis=1, keepdims=True))
        probs = jnp.exp2(masked - new)
        fade = jnp.exp2(old - new)
        tops[rows, :] = jnp.broadcast_to(new, (ROWS, 128))
        sums[rows, :] = sums[rows, :] * fade + jnp.sum(probs, axis=1, keepdims=True)
        acc[rows, :] = acc[rows, :] * fade + jnp.dot(
            probs.astype(BF), vals, preferred_element_type=F32
        )

    def over_tiles(body):
        def turn(tile, carry):
            body(tile)
            return carry

        lax.fori_loop(0, 1024 // ROWS, turn, 0)

    over_tiles(setup)
    for back, blocks, arrays in planes:
        if back == 0:
            over_tiles(lambda tile: step(tile, back, blocks, arrays))
        else:

            last = [ref[...] if blocks == 1 else ref[3] for ref in arrays]
            latest = jnp.max(jnp.maximum(*[p[HALF : HALF + 1, 0:128].astype(F32) for p in last]))

            @pl.when((z >= back) & (latest >= least))
            def _():
                over_tiles(lambda tile: step(tile, back, blocks, arrays))

    if last_call:
        one = acc[0:512, :] / sums[0:512, :]
        two = acc[512:1024, :] / sums[512:1024, :]
        head = one - lam[0:1, :] * two
        scale = lax.rsqrt(jnp.mean(head * head, axis=1, keepdims=True) + 1e-5)
        out[...] = (head * scale * gain[...] * HEAD_SCALE).astype(BF)


def attend(pos, queries, docs, planes, state=None, finish=None):
    kinds = tuple((back, blocks) for back, blocks, _ in planes)
    operands = [queries, docs]
    if finish is not None:
        operands += list(finish)
    if state is not None:
        operands += list(state)
    for _, _, arrays in planes:
        operands += list(arrays)
    big = jax.ShapeDtypeStruct((1024, 128), F32)
    kernel = partial(attend_kernel, kinds, state is None, finish is not None)
    keys = sum(blocks * TOK for _, blocks in kinds)
    if finish is not None:
        outs = jax.ShapeDtypeStruct((512, 128), BF)
        scratch = [pltpu.VMEM((1024, 128), F32)] * 3
    else:
        outs = (big, big, big)
        scratch = []
    return call(kernel, [pos], operands, outs, scratch, flops=1024 * keys * 512)


def project_kernel(pos, attn, resid, gain, *refs):
    weights, (mixed, normed) = refs[:-2], refs[-2:]
    y, core = pos[2], pos[3]
    total = resid[...].astype(F32)
    order = []
    for flip in range(2):
        for ahead, w in zip((0, 3, 1, 2), weights[4 * flip : 4 * flip + 4]):
            order.append((w, ahead, flip))
    for w, ahead, flip in order:
        src = (y + ahead) & 3
        head = 2 * (core ^ flip)
        lhs = jnp.concatenate([attn[head * 4 + src], attn[(head + 1) * 4 + src]], axis=1)
        total = total + jnp.dot(lhs, w[...], preferred_element_type=F32)
    mixed[...] = total
    scale = lax.rsqrt(jnp.mean(total * total, axis=1, keepdims=True) + 1e-6)
    normed[...] = (total * scale * gain[...]).astype(BF)


def route_kernel(pos, routes, weights, pick, high, low):
    core = pos[3]
    group = pos[2] * NC + core
    at = iota((TOK, TOK), 1)
    token = ((at >> 5) & 3) * 64 + 32 * (core ^ (at >> 7)) + (at & 31)
    order = (iota((TOK, TOK), 0) == token).astype(F32)

    def arranged(table):
        return lax.dot_general(
            table,
            order,
            (((0,), (0,)), ((), ())),
            preferred_element_type=F32,
            precision=lax.Precision.HIGHEST,
        )

    ids = arranged(routes[...].astype(F32)).astype(jnp.int32)
    gain = arranged(weights[...])
    target = iota((NZ * NX, TOK), 0) * (NY * NC) + group
    hits = jnp.zeros((NZ * NX, TOK), F32)
    gains = jnp.zeros((NZ * NX, TOK), F32)
    for k in range(4):
        same = ids[k : k + 1, :] == target
        hits = hits + jnp.where(same, 1.0, 0.0)
        gains = gains + jnp.where(same, gain[k : k + 1, :], 0.0)
    before = (iota((TOK, TOK), 0) < iota((TOK, TOK), 1)).astype(BF)
    rank = jnp.dot(hits.astype(BF), before, preferred_element_type=F32)
    rank = jnp.where(hits > 0.5, rank, -1.0)
    slot = iota((NZ * NX, CAP, TOK), 1).astype(F32)
    chosen = (jnp.broadcast_to(rank[:, None, :], (NZ * NX, CAP, TOK)) == slot).reshape(SLOTS, TOK)
    spread = jnp.broadcast_to(gains[:, None, :], (NZ * NX, CAP, TOK)).reshape(SLOTS, TOK)
    pick[...] = jnp.where(chosen, 1.0, 0.0).astype(BF)
    full = jnp.where(chosen, spread, 0.0).T
    upper = full.astype(BF)
    high[...] = upper
    low[...] = (full - upper.astype(F32)).astype(BF)


def dispatch_kernel(pos, pick, *refs):
    chunks, (outgoing, rows) = refs[:-2], refs[-2:]
    y = pos[2]
    for flip in range(2):
        for ahead, ref in zip((0, 3, 1, 2), chunks[4 * flip : 4 * flip + 4]):
            src = (y + ahead) & 3
            rows[pl.ds(pl.multiple_of(flip * HALF + src * 32, 32), 32), :] = ref[...]
    outgoing[...] = jnp.dot(pick[...], rows[...], preferred_element_type=F32).astype(BF)


def shared_kernel(rows, gate, up, down, out):
    gated = jnp.dot(rows[...], gate[...], preferred_element_type=F32)
    lifted = jnp.dot(rows[...], up[...], preferred_element_type=F32)
    act = (gated / (1.0 + jnp.exp(-gated)) * lifted).astype(BF)
    out[...] = jnp.dot(act, down[...], preferred_element_type=F32)


def expert_kernel(rows, gate, up, down, out, acc):
    step = pl.program_id(0)
    gated = jnp.dot(rows[...], gate[0], preferred_element_type=F32)
    lifted = jnp.dot(rows[...], up[0], preferred_element_type=F32)
    act = (gated / (1.0 + jnp.exp(-gated)) * lifted).astype(BF)
    piece = jnp.dot(act, down[0], preferred_element_type=F32)

    @pl.when(step == 0)
    def _():
        acc[...] = piece

    @pl.when(step == 1)
    def _():
        out[...] = (acc[...] + piece).astype(BF)


def experts(rows, gate, up, down):
    width = gate.shape[2] // 2
    whole = pl.BlockSpec((SLOTS, D), lambda i: (0, 0))
    return pl.pallas_call(
        expert_kernel,
        grid=(2,),
        out_shape=jax.ShapeDtypeStruct((SLOTS, D), BF),
        in_specs=[
            whole,
            pl.BlockSpec((1, D, width), lambda i: (0, 0, i)),
            pl.BlockSpec((1, D, width), lambda i: (0, 0, i)),
            pl.BlockSpec((1, width, D), lambda i: (0, i, 0)),
        ],
        out_specs=whole,
        scratch_shapes=[pltpu.VMEM((SLOTS, D), F32)],
        compiler_params=pltpu.CompilerParams(vmem_limit_bytes=VLIM),
        cost_estimate=pl.CostEstimate(
            flops=2 * SLOTS * D * 1536, bytes_accessed=0, transcendentals=0
        ),
        name="expert",
    )(rows, gate, up, down)


def combine_kernel(high, low, rows, shared, keep, send):
    total = (
        jnp.dot(high[...], rows[...], preferred_element_type=F32)
        + jnp.dot(low[...], rows[...], preferred_element_type=F32)
        + shared[...]
    ).astype(BF)
    keep[...] = total[:HALF]
    send[...] = total[HALF:]


def layer(
    resid,
    query_one,
    query_two,
    key_one,
    key_two,
    values,
    documents,
    mix_lambda,
    head_gain,
    out_weight,
    ffn_gain,
    routes,
    route_weight,
    expert_gate,
    expert_up,
    expert_down,
    shared_gate,
    shared_up,
    shared_down,
):
    iz, ix, iy, ic = (lax.axis_index(a) for a in ("z", "x", "y", "c"))
    pos = jnp.stack([iz, ix, iy, ic, jnp.int32(0)])
    plane_axes = ("z", "x")

    any_space = pl.BlockSpec(memory_space=pltpu.HBM)
    packed = pl.pallas_call(
        pack_kernel,
        out_shape=tuple(jax.ShapeDtypeStruct((LINES, 384), BF) for _ in range(4)),
        in_specs=[SMEM, SMEM, VMEM] + [any_space] * 5,
        out_specs=(VMEM,) * 4,
        scratch_shapes=[pltpu.VMEM((TOK, HALF), BF)] * 4
        + [pltpu.VMEM((TOK, 256), BF), pltpu.SemaphoreType.DMA((5,))],
        compiler_params=pltpu.CompilerParams(vmem_limit_bytes=62 * 1024 * 1024),
        name="pack",
    )(pos, mix_lambda, documents.reshape(1, TOK), query_one, query_two, key_one, key_two, values)

    def turn_pairs(turn):
        pairs = []
        for x in range(NX):
            for c in range(NC):
                index = x ^ turn
                pairs.append((x * NC + c, (2 * c + (index >> 1)) * NC + (index & 1)))
        return pairs

    came = [lax.ppermute(packed[t], ("x", "c"), turn_pairs(t)) for t in range(4)]
    keys0, edge, queries, docs, lam = call(
        unpack_kernel,
        [pos],
        came,
        (
            jax.ShapeDtypeStruct((NX, LINES, 256), BF),
            jax.ShapeDtypeStruct((LINES, 256), BF),
            jax.ShapeDtypeStruct((1024, 128), BF),
            jax.ShapeDtypeStruct((1024, 128), F32),
            jax.ShapeDtypeStruct((8, 128), F32),
        ),
    )
    table = jax.ShapeDtypeStruct((SLOTS, TOK), BF)
    pick, weight_high, weight_low = call(
        route_kernel, [pos], [routes, route_weight], (table, table, table)
    )

    queries = after(queries, pick, weight_high, weight_low)
    keys1 = shift(keys0, "z", 1)
    back3 = shift(edge, "z", -3)
    state = attend(pos, queries, docs, [(0, 4, [keys0, swap(keys0)])])
    keys2 = shift(keys1, "z", 1)
    state = attend(pos, queries, docs, [(1, 4, [keys1, swap(keys1)])], state)
    keys3 = shift(keys2, "z", 1)
    pair5 = [back3, swap(back3)]
    state = attend(pos, queries, docs, [(2, 4, [keys2, swap(keys2)]), (5, 1, pair5)], state)
    keys4 = shift(keys3, "z", 1)
    state = attend(pos, queries, docs, [(3, 4, [keys3, swap(keys3)])], state)
    heads = attend(
        pos,
        queries,
        docs,
        [(4, 4, [keys4, swap(keys4)])],
        state,
        finish=(lam, head_gain.reshape(1, 128)),
    )

    held = after(out_weight, packed[0])
    mine = [out_weight] + [shift(held, "y", k) for k in (1, -1, 2)]
    full_weight = mine + [swap(after(w, heads)) for w in mine]

    attn = lax.all_to_all(
        heads.reshape(NX * NY, 32, 128), ("x", "y"), split_axis=0, concat_axis=0, tiled=True
    )
    own_start = (iy * NC + ic) * 32
    resid_own = lax.dynamic_slice_in_dim(resid, own_start, 32, 0)
    mixed, normed = call(
        project_kernel,
        [pos],
        [attn, resid_own, ffn_gain.reshape(1, D)] + full_weight,
        (
            jax.ShapeDtypeStruct((32, D), F32),
            jax.ShapeDtypeStruct((32, D), BF),
        ),
        flops=2 * 32 * D * D,
    )

    chunks = [normed] + [shift(normed, "y", k) for k in (1, -1, 2)]
    chunks = chunks + [swap(c) for c in chunks]
    outgoing, rows = call(
        dispatch_kernel,
        [pos],
        [pick] + chunks,
        (jax.ShapeDtypeStruct((SLOTS, D), BF), jax.ShapeDtypeStruct((TOK, D), BF)),
        flops=2 * SLOTS * TOK * D,
    )
    arrived = lax.all_to_all(
        outgoing.reshape(NZ * NX, CAP, D), plane_axes, split_axis=0, concat_axis=0, tiled=True
    )
    shared = call(
        shared_kernel,
        [],
        [rows, shared_gate, shared_up, shared_down],
        jax.ShapeDtypeStruct((TOK, D), F32),
        flops=2 * TOK * D * 192,
    )
    result = experts(arrived.reshape(SLOTS, D), expert_gate, expert_up, expert_down)
    returned = lax.all_to_all(
        result.reshape(NZ * NX, CAP, D), plane_axes, split_axis=0, concat_axis=0, tiled=True
    ).reshape(SLOTS, D)
    part = jax.ShapeDtypeStruct((HALF, D), BF)
    keep, send = call(
        combine_kernel,
        [],
        [weight_high, weight_low, returned, shared],
        (part, part),
        flops=4 * SLOTS * TOK * D,
    )
    pair_sum = (keep.astype(F32) + swap(send).astype(F32)).astype(BF)
    ffn = lax.all_to_all(
        pair_sum.reshape(NY, 32, D), "y", split_axis=0, concat_axis=0, tiled=True
    )
    return (mixed + ffn.astype(F32).sum(axis=0)).astype(BF)


def solution(mesh):
    split = Mesh(mesh.devices.reshape(NZ, NX, NY, NC), ("z", "x", "y", "c"))
    sp, tp, both = ("z", "x"), ("y", "c"), ("z", "x", "y", "c")
    placed = (
        P(sp, None),
        P(sp, tp),
        P(sp, tp),
        P(sp, tp),
        P(sp, tp),
        P(sp, tp),
        P(sp),
        P(tp),
        P(),
        P(tp, None),
        P(),
        P(sp, None),
        P(sp, None),
        P(both, None, None),
        P(both, None, None),
        P(both, None, None),
        P(None, tp),
        P(None, tp),
        P(tp, None),
    )
    return jax.shard_map(
        layer, mesh=split, in_specs=placed, out_specs=P(both, None), check_vma=False
    )
```

```python
from functools import partial

import jax
import jax.numpy as jnp
from jax import lax
from jax.experimental import pallas as pl
from jax.experimental.pallas import tpu as pltpu
from jax.sharding import Mesh, PartitionSpec as P


NEG_FILL = -1e30
HEAD_SCALE = 0.8
NZ, NX, NY, NC = 8, 4, 4, 2
TOK = 256
D = 2048
HALF = 128
CAP = 8
SLOTS = NZ * NX * CAP
LOG2E = 1.4426950408889634
BF = jnp.bfloat16
F32 = jnp.float32
SMEM = pl.BlockSpec(memory_space=pltpu.SMEM)
VMEM = pl.BlockSpec(memory_space=pltpu.VMEM)
VLIM = 20 * 1024 * 1024


def shift(value, axis, step):
    size = lax.axis_size(axis)
    return lax.ppermute(value, axis, [(i, (i + step) % size) for i in range(size)])


def swap(value):
    return shift(value, "c", 1)


def after(value, *others):
    return lax.optimization_barrier((value, *others))[0]


def call(kernel, scalars, operands, outs, scratch=(), flops=0):
    return pl.pallas_call(
        kernel,
        out_shape=outs,
        in_specs=[SMEM] * len(scalars) + [VMEM] * len(operands),
        out_specs=jax.tree.map(lambda _: VMEM, outs),
        scratch_shapes=list(scratch),
        compiler_params=pltpu.CompilerParams(vmem_limit_bytes=VLIM),
        cost_estimate=pl.CostEstimate(flops=flops, bytes_accessed=0, transcendentals=0),
    )(*scalars, *operands)


def iota(shape, dim):
    return lax.broadcasted_iota(jnp.int32, shape, dim)


LINES = HALF + 8


def pack_kernel(pos, lam, docs, q1, q2, k1, k2, v, *rest):
    outs, (q1v, q2v, k1v, k2v, vv, sems) = rest[:4], rest[4:]
    pairs = ((q1, q1v), (q2, q2v), (k1, k1v), (k2, k2v), (v, vv))
    loads = [pltpu.make_async_copy(a, b, sems.at[i]) for i, (a, b) in enumerate(pairs)]
    for load in loads:
        load.start()
    x = pos[1]
    row = iota((128, 128), 0)
    col = iota((128, 128), 1)
    place = iota((TOK, 128), 0)
    lane = iota((TOK, 128), 1)
    line = iota((8, 128), 0)
    numbers = jnp.broadcast_to(docs[...].astype(F32), (8, TOK)).astype(BF)
    for load in loads:
        load.wait()
    for turn, out in enumerate(outs):
        index = x ^ turn
        head = index >> 1
        core = index & 1
        first = ((col < 64) & (row == col + 64 * head)).astype(BF)
        second = ((col >= 64) & (row == col - 64 + 64 * head)).astype(BF)

        def rows(ref, lanes):
            return jnp.concatenate(
                [
                    ref[pl.ds(pl.multiple_of(64 * i + 32 * core, 32), 32), lanes]
                    for i in range(4)
                ],
                axis=0,
            )

        every = slice(None)

        def merged(a, b):
            return (
                jnp.dot(rows(a, every), first, preferred_element_type=F32)
                + jnp.dot(rows(b, every), second, preferred_element_type=F32)
            ).astype(BF)

        out[0:HALF, 0:128] = merged(q1v, q2v)
        out[0:HALF, 128:256] = merged(k1v, k2v)
        out[0:HALF, 256:384] = rows(vv, pl.ds(pl.multiple_of(128 * head, 128), 128))
        taken = (place == 64 * (lane >> 5) + 32 * core + (lane & 31)).astype(BF)
        own_docs = jnp.dot(numbers, taken, preferred_element_type=F32)
        mixing = jnp.where(head == 0, lam[0], lam[1])
        mixing = jnp.full((8, 128), mixing, F32)
        upper = mixing.astype(BF).astype(F32)
        middle = (mixing - upper).astype(BF).astype(F32)
        lower = mixing - upper - middle
        extra = jnp.where(
            line == 0,
            own_docs,
            jnp.where(line == 1, upper, jnp.where(line == 2, middle, lower)),
        ).astype(BF)
        out[HALF:LINES, 0:128] = extra
        out[HALF:LINES, 128:256] = extra
        out[HALF:LINES, 256:384] = extra


def unpack_kernel(pos, r0, r1, r2, r3, keys, edge, queries, docs, lam):
    mine = (pos[1] & 1) * 2 + pos[3]
    lane = iota((HALF, 128), 1)
    for turn, ref in enumerate((r0, r1, r2, r3)):
        block = mine ^ turn
        keys[block] = ref[:, 128:384]

        @pl.when(block == NX - 1)
        def _():
            edge[...] = ref[:, 128:384]

        both = ref[0:HALF, 0:128]
        start = pl.multiple_of(block * HALF, HALF)
        queries[pl.ds(start, HALF), :] = jnp.where(lane < 64, both, jnp.zeros_like(both))
        queries[pl.ds(start + 512, HALF), :] = jnp.where(lane < 64, jnp.zeros_like(both), both)
        extra = ref[HALF:LINES, 0:128].astype(F32)
        numbers = jnp.broadcast_to(extra[0:1, :], (8, HALF))
        docs[:, pl.ds(start, HALF)] = numbers
        docs[:, pl.ds(start + 512, HALF)] = numbers
        if turn == 0:
            total = extra[1:2, :] + extra[2:3, :] + extra[3:4, :]
            lam[...] = jnp.broadcast_to(total, (8, 128))


COLS = 256


def attend_kernel(kinds, first_call, last_call, pos, *refs):
    refs = list(refs)
    queries, query_docs = refs[0], refs[1]
    at = 2
    if last_call:
        lam, gain = refs[at], refs[at + 1]
        at += 2
    if not first_call:
        state_in = refs[at : at + 3]
        at += 3
    planes = []
    for back, blocks in kinds:
        planes.append((back, blocks, refs[at : at + 2]))
        at += 2
    if last_call:
        out = refs[at]
        tops, sums, acc = refs[at + 1 : at + 4]
        at += 4
    else:
        tops, sums, acc = refs[at : at + 3]
        at += 3
    flipped, key_docs = refs[at : at + 2]
    z, core = pos[0], pos[3]
    if first_call:
        tops[...] = jnp.full((8, 1024), NEG_FILL, F32)
        sums[...] = jnp.zeros((8, 1024), F32)
        acc[...] = jnp.zeros((128, 1024), F32)
    else:
        for dst, src in zip((tops, sums, acc), state_in):
            dst[...] = src[...]

    def visit(back, blocks, arrays):
        count = blocks * TOK
        unit = (iota((HALF, 128), 0) == iota((HALF, 128), 1)).astype(BF)
        parts = [
            ref[:, :] if blocks == 1 else ref[b] for b in range(blocks) for ref in arrays
        ]
        for index, part in enumerate(parts):
            spread = jnp.broadcast_to(part[HALF : HALF + 1, 0:128].astype(F32), (HALF, 128))
            key_docs[index * HALF : (index + 1) * HALF, :] = lax.dot_general(
                unit, spread.astype(BF), (((1,), (1,)), ((), ())), preferred_element_type=F32
            )
            flipped[:, index * HALF : (index + 1) * HALF] = part[0:HALF, 128:256].T
        keys = jnp.concatenate([p[0:HALF, 0:128] for p in parts], axis=0)

        def tile(step, carry):
            cols = pl.ds(pl.multiple_of(step * COLS, COLS), COLS)
            raw = lax.dot_general(
                keys, queries[cols, :], (((1,), (1,)), ((), ())), preferred_element_type=F32
            )
            scaled = raw * (0.125 * LOG2E)
            numbers = key_docs[0:count, :]
            numbers = jnp.concatenate([numbers] * (COLS // 128), axis=1)
            allowed = numbers == query_docs[0:1, cols]
            if back == 0:
                at_key = iota((count, 1), 0)
                line = at_key & 127
                key_pos = (
                    (at_key >> 8) * TOK
                    + 64 * (line >> 5)
                    + 32 * (core ^ ((at_key >> 7) & 1))
                    + (line & 31)
                )
                at_query = (iota((1, COLS), 1) + step * COLS) & 511
                line = at_query & 127
                query_pos = (at_query >> 7) * TOK + 64 * (line >> 5) + 32 * core + (line & 31)
                allowed = allowed & (key_pos <= query_pos)
            masked = jnp.where(allowed, scaled, NEG_FILL)
            old = tops[0:1, cols]
            new = jnp.maximum(old, jnp.max(masked, axis=0, keepdims=True))
            probs = jnp.exp2(masked - new)
            fade = jnp.exp2(old - new)
            total = sums[0:1, cols] * fade + jnp.sum(probs, axis=0, keepdims=True)
            tops[:, cols] = jnp.broadcast_to(new, (8, COLS))
            sums[:, cols] = jnp.broadcast_to(total, (8, COLS))
            acc[:, cols] = acc[:, cols] * fade + jnp.dot(
                flipped[:, 0:count], probs.astype(BF), preferred_element_type=F32
            )
            return carry

        lax.fori_loop(0, 1024 // COLS, tile, 0)

    least = jnp.min(query_docs[0:1, 0:128])
    for back, blocks, arrays in planes:
        if back == 0:
            visit(back, blocks, arrays)
        else:
            last = [ref[...] if blocks == 1 else ref[3] for ref in arrays]
            latest = jnp.max(jnp.maximum(*[p[HALF : HALF + 1, 0:128].astype(F32) for p in last]))

            @pl.when((z >= back) & (latest >= least))
            def _():
                visit(back, blocks, arrays)

    if last_call:
        one = acc[:, 0:512] / sums[0:1, 0:512]
        two = acc[:, 512:1024] / sums[0:1, 512:1024]
        head = one - lam[0:1, 0:1] * two
        scale = lax.rsqrt(jnp.mean(head * head, axis=0, keepdims=True) + 1e-5)
        out[...] = ((head * scale).T * gain[...] * HEAD_SCALE).astype(BF)


def attend(pos, queries, docs, planes, state=None, finish=None):
    kinds = tuple((back, blocks) for back, blocks, _ in planes)
    operands = [queries, docs]
    if finish is not None:
        operands += list(finish)
    if state is not None:
        operands += list(state)
    for _, _, arrays in planes:
        operands += list(arrays)
    row = jax.ShapeDtypeStruct((8, 1024), F32)
    big = (row, row, jax.ShapeDtypeStruct((128, 1024), F32))
    work = [pltpu.VMEM((128, 1024), BF), pltpu.VMEM((1024, 128), F32)]
    kernel = partial(attend_kernel, kinds, state is None, finish is not None)
    keys = sum(blocks * TOK for _, blocks in kinds)
    if finish is not None:
        outs = jax.ShapeDtypeStruct((512, 128), BF)
        scratch = [pltpu.VMEM(b.shape, F32) for b in big] + work
    else:
        outs = big
        scratch = work
    return call(kernel, [pos], operands, outs, scratch, flops=1024 * keys * 512)


def project_kernel(pos, attn, resid, gain, *refs):
    weights = refs[:8]
    mixed, normed, held, left, sums, sems = refs[8:]
    y, core = pos[2], pos[3]
    for index, w in enumerate(weights):
        pltpu.make_async_copy(w, held.at[index], sems.at[index]).start()
    for index in range(8):
        src = (y + (0, 3, 1, 2)[index % 4]) & 3
        head = 2 * (core ^ (index // 4))
        left[index] = jnp.concatenate([attn[head * 4 + src], attn[(head + 1) * 4 + src]], axis=1)
    sums[...] = resid[...].astype(F32)

    def turn(index, carry):
        pltpu.make_async_copy(weights[0], held.at[index], sems.at[index]).wait()
        sums[...] += jnp.dot(left[index], held[index], preferred_element_type=F32)
        return carry

    lax.fori_loop(0, 8, turn, 0)
    total = sums[...]
    mixed[...] = total
    scale = lax.rsqrt(jnp.mean(total * total, axis=1, keepdims=True) + 1e-6)
    normed[...] = (total * scale * gain[...]).astype(BF)


def route_kernel(pos, routes, weights, pick, tables):
    core = pos[3]
    group = pos[2] * NC + core
    at = iota((TOK, TOK), 1)
    token = ((at >> 5) & 3) * 64 + 32 * (core ^ (at >> 7)) + (at & 31)
    order = (iota((TOK, TOK), 0) == token).astype(F32)

    def arranged(table):
        return lax.dot_general(
            table,
            order,
            (((0,), (0,)), ((), ())),
            preferred_element_type=F32,
            precision=lax.Precision.HIGHEST,
        )

    ids = arranged(routes[...].astype(F32)).astype(jnp.int32)
    gain = arranged(weights[...])
    target = iota((NZ * NX, TOK), 0) * (NY * NC) + group
    hits = jnp.zeros((NZ * NX, TOK), F32)
    gains = jnp.zeros((NZ * NX, TOK), F32)
    for k in range(4):
        same = ids[k : k + 1, :] == target
        hits = hits + jnp.where(same, 1.0, 0.0)
        gains = gains + jnp.where(same, gain[k : k + 1, :], 0.0)
    before = (iota((TOK, TOK), 0) < iota((TOK, TOK), 1)).astype(BF)
    rank = jnp.dot(hits.astype(BF), before, preferred_element_type=F32)
    rank = jnp.where(hits > 0.5, rank, -1.0)
    slot = iota((NZ * NX, CAP, TOK), 1).astype(F32)
    chosen = (jnp.broadcast_to(rank[:, None, :], (NZ * NX, CAP, TOK)) == slot).reshape(SLOTS, TOK)
    spread = jnp.broadcast_to(gains[:, None, :], (NZ * NX, CAP, TOK)).reshape(SLOTS, TOK)
    pick[...] = jnp.where(chosen, 1.0, 0.0).astype(BF)
    full = jnp.where(chosen, spread, 0.0).T
    upper = full.astype(BF)
    tables[:, 0:SLOTS] = upper
    tables[:, SLOTS : 2 * SLOTS] = (full - upper.astype(F32)).astype(BF)


def dispatch_kernel(pos, pick, *refs):
    chunks, (outgoing, rows) = refs[:-2], refs[-2:]
    y = pos[2]
    for flip in range(2):
        for ahead, ref in zip((0, 3, 1, 2), chunks[4 * flip : 4 * flip + 4]):
            src = (y + ahead) & 3
            rows[pl.ds(pl.multiple_of(flip * HALF + src * 32, 32), 32), :] = ref[...]
    outgoing[...] = jnp.dot(pick[...], rows[...], preferred_element_type=F32).astype(BF)


def shared_kernel(rows, gate, up, down, tables, out):
    out[:, D:] = tables[...]

    def turn(index, carry):
        part = pl.ds(pl.multiple_of(index * 64, 64), 64)
        gated = jnp.dot(rows[part, :], gate[...], preferred_element_type=F32)
        lifted = jnp.dot(rows[part, :], up[...], preferred_element_type=F32)
        act = (gated / (1.0 + jnp.exp(-gated)) * lifted).astype(BF)
        out[part, 0:D] = jnp.dot(act, down[...], preferred_element_type=F32).astype(BF)
        return carry

    lax.fori_loop(0, TOK // 64, turn, 0)


def expert_kernel(rows, gate, up, down, out, acc):
    step = pl.program_id(0)
    gated = jnp.dot(rows[...], gate[0], preferred_element_type=F32)
    lifted = jnp.dot(rows[...], up[0], preferred_element_type=F32)
    act = (gated / (1.0 + jnp.exp(-gated)) * lifted).astype(BF)
    piece = jnp.dot(act, down[0], preferred_element_type=F32)

    @pl.when(step == 0)
    def _():
        acc[...] = piece

    @pl.when(step == 1)
    def _():
        out[...] = (acc[...] + piece).astype(BF)


def experts(rows, gate, up, down):
    width = gate.shape[2] // 2
    whole = pl.BlockSpec((SLOTS, D), lambda i: (0, 0))
    return pl.pallas_call(
        expert_kernel,
        grid=(2,),
        out_shape=jax.ShapeDtypeStruct((SLOTS, D), BF),
        in_specs=[
            whole,
            pl.BlockSpec((1, D, width), lambda i: (0, 0, i)),
            pl.BlockSpec((1, D, width), lambda i: (0, 0, i)),
            pl.BlockSpec((1, width, D), lambda i: (0, i, 0)),
        ],
        out_specs=whole,
        scratch_shapes=[pltpu.VMEM((SLOTS, D), F32)],
        compiler_params=pltpu.CompilerParams(vmem_limit_bytes=VLIM),
        cost_estimate=pl.CostEstimate(
            flops=2 * SLOTS * D * 1536, bytes_accessed=0, transcendentals=0
        ),
        name="expert",
    )(rows, gate, up, down)


def combine_kernel(rows, shared, keep, send):
    total = (
        jnp.dot(shared[:, D : D + SLOTS], rows[...], preferred_element_type=F32)
        + jnp.dot(shared[:, D + SLOTS :], rows[...], preferred_element_type=F32)
        + shared[:, 0:D].astype(F32)
    ).astype(BF)
    keep[...] = total[:HALF]
    send[...] = total[HALF:]


def pair_kernel(pos, keep, got, *outs):
    y = pos[2]
    for ahead, out in zip((0, 1, 3, 2), outs):
        rows = pl.ds(pl.multiple_of(((y + ahead) & 3) * 32, 32), 32)
        out[...] = (keep[rows, :].astype(F32) + got[rows, :].astype(F32)).astype(BF)


def layer(
    resid,
    query_one,
    query_two,
    key_one,
    key_two,
    values,
    documents,
    mix_lambda,
    head_gain,
    out_weight,
    ffn_gain,
    routes,
    route_weight,
    expert_gate,
    expert_up,
    expert_down,
    shared_gate,
    shared_up,
    shared_down,
):
    iz, ix, iy, ic = (lax.axis_index(a) for a in ("z", "x", "y", "c"))
    pos = jnp.stack([iz, ix, iy, ic, jnp.int32(0)])
    plane_axes = ("z", "x")

    any_space = pl.BlockSpec(memory_space=pltpu.HBM)
    packed = pl.pallas_call(
        pack_kernel,
        out_shape=tuple(jax.ShapeDtypeStruct((LINES, 384), BF) for _ in range(4)),
        in_specs=[SMEM, SMEM, VMEM] + [any_space] * 5,
        out_specs=(VMEM,) * 4,
        scratch_shapes=[pltpu.VMEM((TOK, HALF), BF)] * 4
        + [pltpu.VMEM((TOK, 256), BF), pltpu.SemaphoreType.DMA((5,))],
        compiler_params=pltpu.CompilerParams(vmem_limit_bytes=62 * 1024 * 1024),
        name="pack",
    )(pos, mix_lambda, documents.reshape(1, TOK), query_one, query_two, key_one, key_two, values)

    def turn_pairs(turn):
        pairs = []
        for x in range(NX):
            for c in range(NC):
                index = x ^ turn
                pairs.append((x * NC + c, (2 * c + (index >> 1)) * NC + (index & 1)))
        return pairs

    came = [lax.ppermute(packed[t], ("x", "c"), turn_pairs(t)) for t in range(4)]
    keys0, edge, queries, docs, lam = call(
        unpack_kernel,
        [pos],
        came,
        (
            jax.ShapeDtypeStruct((NX, LINES, 256), BF),
            jax.ShapeDtypeStruct((LINES, 256), BF),
            jax.ShapeDtypeStruct((1024, 128), BF),
            jax.ShapeDtypeStruct((8, 1024), F32),
            jax.ShapeDtypeStruct((8, 128), F32),
        ),
    )
    keys1 = shift(keys0, "z", 1)
    back3 = shift(edge, "z", -3)
    keys6 = shift(keys0, "z", -2)
    state = attend(pos, queries, docs, [(0, 4, [keys0, swap(keys0)])])
    keys2 = shift(keys1, "z", 1)
    keys4 = shift(keys6, "z", -2)
    state = attend(pos, queries, docs, [(1, 4, [keys1, swap(keys1)])], state)
    keys3 = shift(keys2, "z", 1)
    pair5 = [back3, swap(back3)]
    state = attend(pos, queries, docs, [(2, 4, [keys2, swap(keys2)]), (5, 1, pair5)], state)
    state = attend(pos, queries, docs, [(3, 4, [keys3, swap(keys3)])], state)
    heads = attend(
        pos,
        queries,
        docs,
        [(4, 4, [keys4, swap(keys4)])],
        state,
        finish=(lam, head_gain.reshape(1, 128)),
    )

    mine = [out_weight] + [shift(out_weight, "y", k) for k in (1, -1, 2)]
    full_weight = mine + [
        swap(after(out_weight, queries)),
        swap(after(mine[1], heads)),
        swap(after(mine[2], heads)),
        swap(after(mine[3], heads)),
    ]

    attn = lax.all_to_all(
        heads.reshape(NX * NY, 32, 128), ("x", "y"), split_axis=0, concat_axis=0, tiled=True
    )
    own_start = (iy * NC + ic) * 32
    resid_own = lax.dynamic_slice_in_dim(resid, own_start, 32, 0)
    mixed, normed = pl.pallas_call(
        project_kernel,
        out_shape=(jax.ShapeDtypeStruct((32, D), F32), jax.ShapeDtypeStruct((32, D), BF)),
        in_specs=[SMEM] + [VMEM] * 3 + [any_space] * 8,
        out_specs=(VMEM, VMEM),
        scratch_shapes=[
            pltpu.VMEM((8, 256, D), BF),
            pltpu.VMEM((8, 32, 256), BF),
            pltpu.VMEM((32, D), F32),
            pltpu.SemaphoreType.DMA((8,)),
        ],
        compiler_params=pltpu.CompilerParams(vmem_limit_bytes=VLIM),
        cost_estimate=pl.CostEstimate(
            flops=2 * 32 * D * D, bytes_accessed=0, transcendentals=0
        ),
        name="project",
    )(pos, attn, resid_own, ffn_gain.reshape(1, D), *full_weight)

    table = jax.ShapeDtypeStruct((SLOTS, TOK), BF)
    wide = jax.ShapeDtypeStruct((TOK, 2 * SLOTS), BF)
    pick, weights = call(
        route_kernel, [pos], [after(routes, heads), after(route_weight, heads)], (table, wide)
    )

    chunks = [normed] + [shift(normed, "y", k) for k in (1, -1, 2)]
    chunks = chunks + [swap(c) for c in chunks]
    outgoing, rows = call(
        dispatch_kernel,
        [pos],
        [pick] + chunks,
        (jax.ShapeDtypeStruct((SLOTS, D), BF), jax.ShapeDtypeStruct((TOK, D), BF)),
        flops=2 * SLOTS * TOK * D,
    )
    arrived = lax.all_to_all(
        outgoing.reshape(NZ * NX, CAP, D), plane_axes, split_axis=0, concat_axis=0, tiled=True
    )
    shared = call(
        shared_kernel,
        [],
        [rows, shared_gate, shared_up, shared_down, weights],
        jax.ShapeDtypeStruct((TOK, D + 2 * SLOTS), BF),
        flops=2 * TOK * D * 192,
    )
    result = experts(arrived.reshape(SLOTS, D), expert_gate, expert_up, expert_down)
    returned = lax.all_to_all(
        result.reshape(NZ * NX, CAP, D), plane_axes, split_axis=0, concat_axis=0, tiled=True
    ).reshape(SLOTS, D)
    part = jax.ShapeDtypeStruct((HALF, D), BF)
    keep, send = call(
        combine_kernel, [], [returned, shared], (part, part), flops=4 * SLOTS * TOK * D
    )
    chunk = jax.ShapeDtypeStruct((32, D), BF)
    own, ahead, behind, across = call(pair_kernel, [pos], [keep, swap(send)], (chunk,) * 4)
    came = [shift(ahead, "y", 1), shift(behind, "y", -1), shift(across, "y", 2)]
    total = mixed + own.astype(F32)
    for piece in came:
        total = total + piece.astype(F32)
    return total.astype(BF)


def solution(mesh):
    split = Mesh(mesh.devices.reshape(NZ, NX, NY, NC), ("z", "x", "y", "c"))
    sp, tp, both = ("z", "x"), ("y", "c"), ("z", "x", "y", "c")
    placed = (
        P(sp, None),
        P(sp, tp),
        P(sp, tp),
        P(sp, tp),
        P(sp, tp),
        P(sp, tp),
        P(sp),
        P(tp),
        P(),
        P(tp, None),
        P(),
        P(sp, None),
        P(sp, None),
        P(both, None, None),
        P(both, None, None),
        P(both, None, None),
        P(None, tp),
        P(None, tp),
        P(tp, None),
    )
    return jax.shard_map(
        layer, mesh=split, in_specs=placed, out_specs=P(both, None), check_vma=False
    )
```

```python
from functools import partial

import jax
import jax.numpy as jnp
from jax import lax
from jax.experimental import pallas as pl
from jax.experimental.pallas import tpu as pltpu
from jax.sharding import Mesh, PartitionSpec as P


NEG_FILL = -1e30
HEAD_SCALE = 0.8
NZ, NX, NY, NC = 8, 4, 4, 2
TOK = 256
D = 2048
HALF = 128
CAP = 8
SLOTS = NZ * NX * CAP
LOG2E = 1.4426950408889634
BF = jnp.bfloat16
F32 = jnp.float32
SMEM = pl.BlockSpec(memory_space=pltpu.SMEM)
VMEM = pl.BlockSpec(memory_space=pltpu.VMEM)
VLIM = 20 * 1024 * 1024


def shift(value, axis, step):
    size = lax.axis_size(axis)
    return lax.ppermute(value, axis, [(i, (i + step) % size) for i in range(size)])


def swap(value):
    return shift(value, "c", 1)


def after(value, *others):
    return lax.optimization_barrier((value, *others))[0]


def call(kernel, scalars, operands, outs, scratch=(), flops=0):
    return pl.pallas_call(
        kernel,
        out_shape=outs,
        in_specs=[SMEM] * len(scalars) + [VMEM] * len(operands),
        out_specs=jax.tree.map(lambda _: VMEM, outs),
        scratch_shapes=list(scratch),
        compiler_params=pltpu.CompilerParams(vmem_limit_bytes=VLIM),
        cost_estimate=pl.CostEstimate(flops=flops, bytes_accessed=0, transcendentals=0),
    )(*scalars, *operands)


def iota(shape, dim):
    return lax.broadcasted_iota(jnp.int32, shape, dim)


LINES = HALF + 8


def pack_kernel(pos, lam, docs, q1, q2, k1, k2, v, *rest):
    outs, (q1v, q2v, k1v, k2v, vv, sems) = rest[:4], rest[4:]
    pairs = ((q1, q1v), (q2, q2v), (k1, k1v), (k2, k2v), (v, vv))
    loads = [pltpu.make_async_copy(a, b, sems.at[i]) for i, (a, b) in enumerate(pairs)]
    for load in loads:
        load.start()
    x = pos[1]
    row = iota((128, 128), 0)
    col = iota((128, 128), 1)
    place = iota((TOK, 128), 0)
    lane = iota((TOK, 128), 1)
    line = iota((8, 128), 0)
    numbers = jnp.broadcast_to(docs[...].astype(F32), (8, TOK)).astype(BF)
    for load in loads:
        load.wait()
    for turn, out in enumerate(outs):
        index = x ^ turn
        head = index >> 1
        core = index & 1
        first = ((col < 64) & (row == col + 64 * head)).astype(BF)
        second = ((col >= 64) & (row == col - 64 + 64 * head)).astype(BF)

        def rows(ref, lanes):
            return jnp.concatenate(
                [
                    ref[pl.ds(pl.multiple_of(64 * i + 32 * core, 32), 32), lanes]
                    for i in range(4)
                ],
                axis=0,
            )

        every = slice(None)

        def merged(a, b):
            return (
                jnp.dot(rows(a, every), first, preferred_element_type=F32)
                + jnp.dot(rows(b, every), second, preferred_element_type=F32)
            ).astype(BF)

        out[0:HALF, 0:128] = merged(q1v, q2v)
        out[0:HALF, 128:256] = merged(k1v, k2v)
        out[0:HALF, 256:384] = rows(vv, pl.ds(pl.multiple_of(128 * head, 128), 128))
        taken = (place == 64 * (lane >> 5) + 32 * core + (lane & 31)).astype(BF)
        own_docs = jnp.dot(numbers, taken, preferred_element_type=F32)
        mixing = jnp.where(head == 0, lam[0], lam[1])
        mixing = jnp.full((8, 128), mixing, F32)
        upper = mixing.astype(BF).astype(F32)
        middle = (mixing - upper).astype(BF).astype(F32)
        lower = mixing - upper - middle
        extra = jnp.where(
            line == 0,
            own_docs,
            jnp.where(line == 1, upper, jnp.where(line == 2, middle, lower)),
        ).astype(BF)
        out[HALF:LINES, 0:128] = extra
        out[HALF:LINES, 128:256] = extra
        out[HALF:LINES, 256:384] = extra


def unpack_kernel(pos, r0, r1, r2, r3, keys, queries, docs, lam):
    mine = (pos[1] & 1) * 2 + pos[3]
    lane = iota((HALF, 128), 1)
    for turn, ref in enumerate((r0, r1, r2, r3)):
        block = mine ^ turn
        keys[block] = ref[:, 128:384]
        both = ref[0:HALF, 0:128]
        start = pl.multiple_of(block * HALF, HALF)
        queries[pl.ds(start, HALF), :] = jnp.where(lane < 64, both, jnp.zeros_like(both))
        queries[pl.ds(start + 512, HALF), :] = jnp.where(lane < 64, jnp.zeros_like(both), both)
        extra = ref[HALF:LINES, 0:128].astype(F32)
        numbers = jnp.broadcast_to(extra[0:1, :], (8, HALF))
        docs[:, pl.ds(start, HALF)] = numbers
        docs[:, pl.ds(start + 512, HALF)] = numbers
        if turn == 0:
            total = extra[1:2, :] + extra[2:3, :] + extra[3:4, :]
            lam[...] = jnp.broadcast_to(total, (8, 128))


COLS = 256


def attend_kernel(kinds, first_call, last_call, pos, *refs):
    refs = list(refs)
    queries, query_docs = refs[0], refs[1]
    at = 2
    if last_call:
        lam, gain = refs[at], refs[at + 1]
        at += 2
    if not first_call:
        state_in = refs[at : at + 3]
        at += 3
    planes = []
    for back, blocks in kinds:
        planes.append((back, blocks, refs[at : at + 2]))
        at += 2
    if last_call:
        out = refs[at]
        tops, sums, acc = refs[at + 1 : at + 4]
        at += 4
    else:
        tops, sums, acc = refs[at : at + 3]
        at += 3
    flipped, key_docs = refs[at : at + 2]
    z, core = pos[0], pos[3]
    if first_call:
        tops[...] = jnp.full((8, 1024), NEG_FILL, F32)
        sums[...] = jnp.zeros((8, 1024), F32)
        acc[...] = jnp.zeros((128, 1024), F32)
    else:
        for dst, src in zip((tops, sums, acc), state_in):
            dst[...] = src[...]

    def visit(back, blocks, arrays):
        count = blocks * TOK
        unit = (iota((HALF, 128), 0) == iota((HALF, 128), 1)).astype(BF)
        parts = [
            ref[:, :] if blocks == 1 else ref[b] for b in range(blocks) for ref in arrays
        ]
        for index, part in enumerate(parts):
            spread = jnp.broadcast_to(part[HALF : HALF + 1, 0:128].astype(F32), (HALF, 128))
            key_docs[index * HALF : (index + 1) * HALF, :] = lax.dot_general(
                unit, spread.astype(BF), (((1,), (1,)), ((), ())), preferred_element_type=F32
            )
            flipped[:, index * HALF : (index + 1) * HALF] = part[0:HALF, 128:256].T
        keys = jnp.concatenate([p[0:HALF, 0:128] for p in parts], axis=0)

        def tile(step, carry):
            cols = pl.ds(pl.multiple_of(step * COLS, COLS), COLS)
            raw = lax.dot_general(
                keys, queries[cols, :], (((1,), (1,)), ((), ())), preferred_element_type=F32
            )
            scaled = raw * (0.125 * LOG2E)
            numbers = key_docs[0:count, :]
            numbers = jnp.concatenate([numbers] * (COLS // 128), axis=1)
            allowed = numbers == query_docs[0:1, cols]
            if back == 0:
                at_key = iota((count, 1), 0)
                line = at_key & 127
                key_pos = (
                    (at_key >> 8) * TOK
                    + 64 * (line >> 5)
                    + 32 * (core ^ ((at_key >> 7) & 1))
                    + (line & 31)
                )
                at_query = (iota((1, COLS), 1) + step * COLS) & 511
                line = at_query & 127
                query_pos = (at_query >> 7) * TOK + 64 * (line >> 5) + 32 * core + (line & 31)
                allowed = allowed & (key_pos <= query_pos)
            masked = jnp.where(allowed, scaled, NEG_FILL)
            old = tops[0:1, cols]
            new = jnp.maximum(old, jnp.max(masked, axis=0, keepdims=True))
            probs = jnp.exp2(masked - new)
            fade = jnp.exp2(old - new)
            total = sums[0:1, cols] * fade + jnp.sum(probs, axis=0, keepdims=True)
            tops[:, cols] = jnp.broadcast_to(new, (8, COLS))
            sums[:, cols] = jnp.broadcast_to(total, (8, COLS))
            acc[:, cols] = acc[:, cols] * fade + jnp.dot(
                flipped[:, 0:count], probs.astype(BF), preferred_element_type=F32
            )
            return carry

        lax.fori_loop(0, 1024 // COLS, tile, 0)

    least = jnp.min(query_docs[0:1, 0:128])
    for back, blocks, arrays in planes:
        if back == 0:
            visit(back, blocks, arrays)
        else:
            last = [ref[...] if blocks == 1 else ref[3] for ref in arrays]
            latest = jnp.max(jnp.maximum(*[p[HALF : HALF + 1, 0:128].astype(F32) for p in last]))

            @pl.when((z >= back) & (latest >= least))
            def _():
                visit(back, blocks, arrays)

    if last_call:
        one = acc[:, 0:512] / sums[0:1, 0:512]
        two = acc[:, 512:1024] / sums[0:1, 512:1024]
        head = one - lam[0:1, 0:1] * two
        scale = lax.rsqrt(jnp.mean(head * head, axis=0, keepdims=True) + 1e-5)
        out[...] = ((head * scale).T * gain[...] * HEAD_SCALE).astype(BF)


def attend(pos, queries, docs, planes, state=None, finish=None):
    kinds = tuple((back, blocks) for back, blocks, _ in planes)
    operands = [queries, docs]
    if finish is not None:
        operands += list(finish)
    if state is not None:
        operands += list(state)
    for _, _, arrays in planes:
        operands += list(arrays)
    row = jax.ShapeDtypeStruct((8, 1024), F32)
    big = (row, row, jax.ShapeDtypeStruct((128, 1024), F32))
    work = [pltpu.VMEM((128, 1024), BF), pltpu.VMEM((1024, 128), F32)]
    kernel = partial(attend_kernel, kinds, state is None, finish is not None)
    keys = sum(blocks * TOK for _, blocks in kinds)
    if finish is not None:
        outs = jax.ShapeDtypeStruct((512, 128), BF)
        scratch = [pltpu.VMEM(b.shape, F32) for b in big] + work
    else:
        outs = big
        scratch = work
    return call(kernel, [pos], operands, outs, scratch, flops=1024 * keys * 512)


def project_kernel(pos, attn, resid, gain, *refs):
    weights = refs[:8]
    mixed, normed, held, left, sums, sems = refs[8:]
    y, core = pos[2], pos[3]
    for index, w in enumerate(weights):
        pltpu.make_async_copy(w, held.at[index], sems.at[index]).start()
    for index in range(8):
        src = (y + (0, 3, 1, 2)[index % 4]) & 3
        head = 2 * (core ^ (index // 4))
        left[index] = jnp.concatenate([attn[head * 4 + src], attn[(head + 1) * 4 + src]], axis=1)
    sums[...] = resid[...].astype(F32)

    def turn(index, carry):
        pltpu.make_async_copy(weights[0], held.at[index], sems.at[index]).wait()
        sums[...] += jnp.dot(left[index], held[index], preferred_element_type=F32)
        return carry

    lax.fori_loop(0, 8, turn, 0)
    total = sums[...]
    mixed[...] = total
    scale = lax.rsqrt(jnp.mean(total * total, axis=1, keepdims=True) + 1e-6)
    normed[...] = (total * scale * gain[...]).astype(BF)


def route_kernel(pos, routes, weights, pick, tables):
    core = pos[3]
    group = pos[2] * NC + core
    at = iota((TOK, TOK), 1)
    token = ((at >> 5) & 3) * 64 + 32 * (core ^ (at >> 7)) + (at & 31)
    order = (iota((TOK, TOK), 0) == token).astype(F32)

    def arranged(table):
        return lax.dot_general(
            table,
            order,
            (((0,), (0,)), ((), ())),
            preferred_element_type=F32,
            precision=lax.Precision.HIGHEST,
        )

    ids = arranged(routes[...].astype(F32)).astype(jnp.int32)
    gain = arranged(weights[...])
    target = iota((NZ * NX, TOK), 0) * (NY * NC) + group
    hits = jnp.zeros((NZ * NX, TOK), F32)
    gains = jnp.zeros((NZ * NX, TOK), F32)
    for k in range(4):
        same = ids[k : k + 1, :] == target
        hits = hits + jnp.where(same, 1.0, 0.0)
        gains = gains + jnp.where(same, gain[k : k + 1, :], 0.0)
    before = (iota((TOK, TOK), 0) < iota((TOK, TOK), 1)).astype(BF)
    rank = jnp.dot(hits.astype(BF), before, preferred_element_type=F32)
    rank = jnp.where(hits > 0.5, rank, -1.0)
    slot = iota((NZ * NX, CAP, TOK), 1).astype(F32)
    chosen = (jnp.broadcast_to(rank[:, None, :], (NZ * NX, CAP, TOK)) == slot).reshape(SLOTS, TOK)
    spread = jnp.broadcast_to(gains[:, None, :], (NZ * NX, CAP, TOK)).reshape(SLOTS, TOK)
    pick[...] = jnp.where(chosen, 1.0, 0.0).astype(BF)
    full = jnp.where(chosen, spread, 0.0).T
    upper = full.astype(BF)
    tables[:, 0:SLOTS] = upper
    tables[:, SLOTS : 2 * SLOTS] = (full - upper.astype(F32)).astype(BF)


def dispatch_kernel(pos, pick, *refs):
    chunks, (outgoing, rows) = refs[:-2], refs[-2:]
    y = pos[2]
    for flip in range(2):
        for ahead, ref in zip((0, 3, 1, 2), chunks[4 * flip : 4 * flip + 4]):
            src = (y + ahead) & 3
            rows[pl.ds(pl.multiple_of(flip * HALF + src * 32, 32), 32), :] = ref[...]
    outgoing[...] = jnp.dot(pick[...], rows[...], preferred_element_type=F32).astype(BF)


def shared_kernel(rows, gate, up, down, tables, out):
    out[:, D:] = tables[...]

    def turn(index, carry):
        part = pl.ds(pl.multiple_of(index * 64, 64), 64)
        gated = jnp.dot(rows[part, :], gate[...], preferred_element_type=F32)
        lifted = jnp.dot(rows[part, :], up[...], preferred_element_type=F32)
        act = (gated / (1.0 + jnp.exp(-gated)) * lifted).astype(BF)
        out[part, 0:D] = jnp.dot(act, down[...], preferred_element_type=F32).astype(BF)
        return carry

    lax.fori_loop(0, TOK // 64, turn, 0)


def expert_kernel(rows, gate, up, down, out, acc):
    step = pl.program_id(0)
    gated = jnp.dot(rows[...], gate[0], preferred_element_type=F32)
    lifted = jnp.dot(rows[...], up[0], preferred_element_type=F32)
    act = (gated / (1.0 + jnp.exp(-gated)) * lifted).astype(BF)
    piece = jnp.dot(act, down[0], preferred_element_type=F32)

    @pl.when(step == 0)
    def _():
        acc[...] = piece

    @pl.when(step == 1)
    def _():
        out[...] = (acc[...] + piece).astype(BF)


def experts(rows, gate, up, down):
    width = gate.shape[2] // 2
    whole = pl.BlockSpec((SLOTS, D), lambda i: (0, 0))
    return pl.pallas_call(
        expert_kernel,
        grid=(2,),
        out_shape=jax.ShapeDtypeStruct((SLOTS, D), BF),
        in_specs=[
            whole,
            pl.BlockSpec((1, D, width), lambda i: (0, 0, i)),
            pl.BlockSpec((1, D, width), lambda i: (0, 0, i)),
            pl.BlockSpec((1, width, D), lambda i: (0, i, 0)),
        ],
        out_specs=whole,
        scratch_shapes=[pltpu.VMEM((SLOTS, D), F32)],
        compiler_params=pltpu.CompilerParams(vmem_limit_bytes=VLIM),
        cost_estimate=pl.CostEstimate(
            flops=2 * SLOTS * D * 1536, bytes_accessed=0, transcendentals=0
        ),
        name="expert",
    )(rows, gate, up, down)


def combine_kernel(rows, shared, keep, send):
    total = (
        jnp.dot(shared[:, D : D + SLOTS], rows[...], preferred_element_type=F32)
        + jnp.dot(shared[:, D + SLOTS :], rows[...], preferred_element_type=F32)
        + shared[:, 0:D].astype(F32)
    ).astype(BF)
    keep[...] = total[:HALF]
    send[...] = total[HALF:]


def pair_kernel(pos, keep, got, *outs):
    y = pos[2]
    for ahead, out in zip((0, 1, 3, 2), outs):
        rows = pl.ds(pl.multiple_of(((y + ahead) & 3) * 32, 32), 32)
        out[...] = (keep[rows, :].astype(F32) + got[rows, :].astype(F32)).astype(BF)


def layer(
    resid,
    query_one,
    query_two,
    key_one,
    key_two,
    values,
    documents,
    mix_lambda,
    head_gain,
    out_weight,
    ffn_gain,
    routes,
    route_weight,
    expert_gate,
    expert_up,
    expert_down,
    shared_gate,
    shared_up,
    shared_down,
):
    iz, ix, iy, ic = (lax.axis_index(a) for a in ("z", "x", "y", "c"))
    pos = jnp.stack([iz, ix, iy, ic, jnp.int32(0)])
    plane_axes = ("z", "x")

    any_space = pl.BlockSpec(memory_space=pltpu.HBM)
    packed = pl.pallas_call(
        pack_kernel,
        out_shape=tuple(jax.ShapeDtypeStruct((LINES, 384), BF) for _ in range(4)),
        in_specs=[SMEM, SMEM, VMEM] + [any_space] * 5,
        out_specs=(VMEM,) * 4,
        scratch_shapes=[pltpu.VMEM((TOK, HALF), BF)] * 4
        + [pltpu.VMEM((TOK, 256), BF), pltpu.SemaphoreType.DMA((5,))],
        compiler_params=pltpu.CompilerParams(vmem_limit_bytes=62 * 1024 * 1024),
        name="pack",
    )(pos, mix_lambda, documents.reshape(1, TOK), query_one, query_two, key_one, key_two, values)

    def turn_pairs(turn):
        pairs = []
        for x in range(NX):
            for c in range(NC):
                index = x ^ turn
                pairs.append((x * NC + c, (2 * c + (index >> 1)) * NC + (index & 1)))
        return pairs

    came = [lax.ppermute(packed[t], ("x", "c"), turn_pairs(t)) for t in range(4)]
    keys0, queries, docs, lam = call(
        unpack_kernel,
        [pos],
        came,
        (
            jax.ShapeDtypeStruct((NX, LINES, 256), BF),
            jax.ShapeDtypeStruct((1024, 128), BF),
            jax.ShapeDtypeStruct((8, 1024), F32),
            jax.ShapeDtypeStruct((8, 128), F32),
        ),
    )
    keys1 = shift(keys0, "z", 1)
    keys6 = shift(keys0, "z", -2)
    state = attend(pos, queries, docs, [(0, 4, [keys0, swap(keys0)])])
    keys2 = shift(keys1, "z", 1)
    back3 = shift(keys6[NX - 1], "z", -1)
    keys4 = shift(keys6, "z", -2)
    state = attend(pos, queries, docs, [(1, 4, [keys1, swap(keys1)])], state)
    keys3 = shift(keys2, "z", 1)
    pair5 = [back3, swap(back3)]
    state = attend(pos, queries, docs, [(2, 4, [keys2, swap(keys2)])], state)
    state = attend(pos, queries, docs, [(3, 4, [keys3, swap(keys3)]), (5, 1, pair5)], state)
    heads = attend(
        pos,
        queries,
        docs,
        [(4, 4, [keys4, swap(keys4)])],
        state,
        finish=(lam, head_gain.reshape(1, 128)),
    )

    mine = [out_weight] + [shift(out_weight, "y", k) for k in (1, -1, 2)]
    full_weight = mine + [
        swap(after(out_weight, queries)),
        swap(after(mine[1], heads)),
        swap(after(mine[2], heads)),
        swap(after(mine[3], heads)),
    ]

    attn = lax.all_to_all(
        heads.reshape(NX * NY, 32, 128), ("x", "y"), split_axis=0, concat_axis=0, tiled=True
    )
    own_start = (iy * NC + ic) * 32
    resid_own = lax.dynamic_slice_in_dim(resid, own_start, 32, 0)
    mixed, normed = pl.pallas_call(
        project_kernel,
        out_shape=(jax.ShapeDtypeStruct((32, D), F32), jax.ShapeDtypeStruct((32, D), BF)),
        in_specs=[SMEM] + [VMEM] * 3 + [any_space] * 8,
        out_specs=(VMEM, VMEM),
        scratch_shapes=[
            pltpu.VMEM((8, 256, D), BF),
            pltpu.VMEM((8, 32, 256), BF),
            pltpu.VMEM((32, D), F32),
            pltpu.SemaphoreType.DMA((8,)),
        ],
        compiler_params=pltpu.CompilerParams(vmem_limit_bytes=VLIM),
        cost_estimate=pl.CostEstimate(
            flops=2 * 32 * D * D, bytes_accessed=0, transcendentals=0
        ),
        name="project",
    )(pos, attn, resid_own, ffn_gain.reshape(1, D), *full_weight)

    table = jax.ShapeDtypeStruct((SLOTS, TOK), BF)
    wide = jax.ShapeDtypeStruct((TOK, 2 * SLOTS), BF)
    pick, weights = call(
        route_kernel, [pos], [after(routes, heads), after(route_weight, heads)], (table, wide)
    )

    chunks = [normed] + [shift(normed, "y", k) for k in (1, -1, 2)]
    chunks = chunks + [swap(c) for c in chunks]
    outgoing, rows = call(
        dispatch_kernel,
        [pos],
        [pick] + chunks,
        (jax.ShapeDtypeStruct((SLOTS, D), BF), jax.ShapeDtypeStruct((TOK, D), BF)),
        flops=2 * SLOTS * TOK * D,
    )
    arrived = lax.all_to_all(
        outgoing.reshape(NZ * NX, CAP, D), plane_axes, split_axis=0, concat_axis=0, tiled=True
    )
    shared = call(
        shared_kernel,
        [],
        [rows, shared_gate, shared_up, shared_down, weights],
        jax.ShapeDtypeStruct((TOK, D + 2 * SLOTS), BF),
        flops=2 * TOK * D * 192,
    )
    result = experts(arrived.reshape(SLOTS, D), expert_gate, expert_up, expert_down)
    returned = lax.all_to_all(
        result.reshape(NZ * NX, CAP, D), plane_axes, split_axis=0, concat_axis=0, tiled=True
    ).reshape(SLOTS, D)
    part = jax.ShapeDtypeStruct((HALF, D), BF)
    keep, send = call(
        combine_kernel, [], [returned, shared], (part, part), flops=4 * SLOTS * TOK * D
    )
    chunk = jax.ShapeDtypeStruct((32, D), BF)
    own, ahead, behind, across = call(pair_kernel, [pos], [keep, swap(send)], (chunk,) * 4)
    came = [shift(ahead, "y", 1), shift(behind, "y", -1), shift(across, "y", 2)]
    total = mixed + own.astype(F32)
    for piece in came:
        total = total + piece.astype(F32)
    return total.astype(BF)


def solution(mesh):
    split = Mesh(mesh.devices.reshape(NZ, NX, NY, NC), ("z", "x", "y", "c"))
    sp, tp, both = ("z", "x"), ("y", "c"), ("z", "x", "y", "c")
    placed = (
        P(sp, None),
        P(sp, tp),
        P(sp, tp),
        P(sp, tp),
        P(sp, tp),
        P(sp, tp),
        P(sp),
        P(tp),
        P(),
        P(tp, None),
        P(),
        P(sp, None),
        P(sp, None),
        P(both, None, None),
        P(both, None, None),
        P(both, None, None),
        P(None, tp),
        P(None, tp),
        P(tp, None),
    )
    return jax.shard_map(
        layer, mesh=split, in_specs=placed, out_specs=P(both, None), check_vma=False
    )
```
